32 devices in a mesh: sp: 8 (over z, x), tp: 4 (over y, core).
Axes of the slice: x: 2, y: 2, z: 4, core: 2. Of those that a mesh axis runs over, the one named last changes fastest.
Arguments:
- tokens: bfloat16 [4096, 2048], P('sp', 'tp'), may hold values from -6 to 6
- norm_gain: float32 [2048], replicated, may hold values from 0.1 to 1.9
- w_query: bfloat16 [2048, 1024], P('sp', 'tp'), may hold values from -1 to 1
- w_key: bfloat16 [2048, 256], P('sp', 'tp'), may hold values from -16 to 16
- w_value: bfloat16 [2048, 256], P('sp', 'tp'), may hold values from -1 to 1
- w_post_gate: bfloat16 [2048, 1024], P('sp', 'tp'), may hold values from -0.125 to 0.125
- w_pre_gate: bfloat16 [2048, 1024], P('sp', 'tp'), may hold values from -0.125 to 0.125
- w_conv_in: bfloat16 [2048, 1024], P('sp', 'tp'), may hold values from -0.125 to 0.125
- conv_taps: float32 [3, 1024], P(None, 'tp'), may hold values from -3 to 3
- sink_logit: float32 [16], P('tp'), may hold values from 2 to 6
- w_out_attn: bfloat16 [1024, 2048], P('tp', 'sp'), may hold values from -0.1875 to 0.1875
- w_out_conv: bfloat16 [1024, 2048], P('tp', 'sp'), may hold values from -0.1875 to 0.1875
Outputs:
- mixed: bfloat16 [4096, 2048], P(('sp', 'tp'))
- log_weight_sum: float32 [16, 4096], P('tp', 'sp')
The draws below stay inside these ranges and needn't reach their ends.
All inputs are finite; a program needn't handle non-finite values.
Results may differ from the reference program's by a relative error of at most 0.012.
The reference program's roundings to bfloat16 on the way count: a program that leaves them out, or rounds other values in their place, can miss the bound.
Values may be sent and summed in bfloat16 or wider, within the bound.
A program may use at most 64 MiB of HBM per device.

```python
import jax
import jax.numpy as jnp
from jax import lax

D = 2048
HEADS = 16
KV_HEADS = 4
HEAD_DIM = 64
CONV_CH = 1024
WINDOW = 128
GRID_W = 64
TOKENS = 4096


def query_key_pair(key):
    base = jax.random.fold_in(key, 11)
    query_seed, key_seed = jax.random.split(base, 2)
    fan_scale = D ** (-0.5)
    w_query = jnp.clip(jax.random.normal(query_seed, (D, HEADS * HEAD_DIM), jnp.float32), -6.0, 6.0) * fan_scale
    w_key = jnp.clip(jax.random.normal(key_seed, (D, KV_HEADS * HEAD_DIM), jnp.float32), -6.0, 6.0) * fan_scale
    return (w_query, w_key)


def draw_w_query(key, part):
    return query_key_pair(key)[0].astype(jnp.bfloat16)


def draw_w_key(key, part):
    return query_key_pair(key)[1].astype(jnp.bfloat16)


def steps_of(stream_key, dims, shards, smallest, high):
    factor_of, own = 1.0, jax.random.fold_in(stream_key, 6)
    for axis_at, blocks in shards:
        draws = jnp.exp(jax.random.uniform(jax.random.fold_in(own, axis_at), (blocks,), jnp.float32, smallest / len(shards), high / len(shards)))
        factor_of = factor_of * jnp.repeat(draws, dims[axis_at] // blocks).reshape([-1 if axis == axis_at else 1 for axis in range(len(dims))])
    return factor_of


def normal_values(key, dims, spread, limit, shards=(), kind=jnp.bfloat16):
    array = jax.random.normal(key, dims, jnp.float32) * spread
    if len(shards) > 0:
        array = steps_of(key, dims, shards, -0.22, 0.18) * array
    return jnp.clip(array, min=-limit, max=limit).astype(kind)


def setup_inputs(seed: int = 0) -> dict:
    streams_of = jax.random.split(jax.random.key(seed), 13)
    return {
        "tokens": normal_values(streams_of[0], (TOKENS, D), 1.0, 6.0, ((0, 8), (1, 4))),
        "norm_gain": jnp.clip(1.0 + 0.18 * jax.random.normal(streams_of[1], (D,), jnp.float32), 0.1, 1.9),
        "w_query": draw_w_query(jax.random.fold_in(streams_of[12], 71), 0),
        "w_key": draw_w_key(jax.random.fold_in(streams_of[12], 71), 0),
        "w_value": normal_values(streams_of[4], (D, KV_HEADS * HEAD_DIM), (D // 64) ** -0.5, 1.0, ((0, 8), (1, 4))),
        "w_post_gate": normal_values(streams_of[5], (D, CONV_CH), D ** -0.5, 0.125, ((0, 8), (1, 4))),
        "w_pre_gate": normal_values(streams_of[6], (D, CONV_CH), D ** -0.5, 0.125, ((0, 8), (1, 4))),
        "w_conv_in": normal_values(streams_of[7], (D, CONV_CH), D ** -0.5, 0.125, ((0, 8), (1, 4))),
        "conv_taps": normal_values(streams_of[8], (3, CONV_CH), 0.6, 3.0, ((1, 4),), jnp.float32),
        "sink_logit": jnp.clip(2.0 + 4.0 * jax.random.uniform(streams_of[9], (HEADS,), jnp.float32) ** steps_of(streams_of[9], (HEADS,), ((0, 4),), -0.2, 0.2), 2.0, 6.0),
        "w_out_attn": normal_values(streams_of[10], (HEADS * HEAD_DIM, D), (HEADS * HEAD_DIM) ** -0.5, 0.1875, ((0, 4), (1, 8))),
        "w_out_conv": normal_values(streams_of[11], (CONV_CH, D), CONV_CH ** -0.5, 0.1875, ((0, 4), (1, 8))),
    }


rope_base = 10000.0
norm_eps = 1e-06

def rotate_pair(values, angles):
    first_half, second_half = jnp.split(values, 2, axis=-1)
    cosine = jnp.cos(angles)[:, None, :]
    sine_part = jnp.sin(angles)[:, None, :]
    return jnp.concatenate([first_half * cosine - second_half * sine_part, first_half * sine_part + second_half * cosine], axis=-1)

def axial_rotate(values, positions):
    half_dim = values.shape[-1] // 2
    inv_freq = rope_base ** (-jnp.arange(0, half_dim, 2).astype(jnp.float32) / half_dim)
    row_angle = (positions // GRID_W).astype(jnp.float32)[:, None] * inv_freq
    col_angle = (positions % GRID_W).astype(jnp.float32)[:, None] * inv_freq
    row_part, col_part = jnp.split(values, 2, axis=-1)
    return jnp.concatenate([rotate_pair(row_part, row_angle), rotate_pair(col_part, col_angle)], axis=-1)

def reference(tokens, norm_gain, w_query, w_key, w_value, w_post_gate, w_pre_gate, w_conv_in, conv_taps, sink_logit, w_out_attn, w_out_conv):
    total_tokens = tokens.shape[0]
    whole = tokens.astype(jnp.float32)
    normed = (whole * lax.rsqrt(lax.optimization_barrier(jnp.mean(whole * whole, axis=1, keepdims=True)) + norm_eps) * norm_gain.astype(jnp.float32)).astype(jnp.bfloat16)

    def project(weight):
        return jnp.dot(normed, weight, preferred_element_type=jnp.float32)
    positions = jnp.arange(total_tokens, dtype=jnp.int32)
    queries = axial_rotate(project(w_query).reshape(total_tokens, HEADS, HEAD_DIM), positions).astype(jnp.bfloat16)
    keys_rot = axial_rotate(project(w_key).reshape(total_tokens, KV_HEADS, HEAD_DIM), positions).astype(jnp.bfloat16)
    values_all = project(w_value).astype(jnp.bfloat16).reshape(total_tokens, KV_HEADS, HEAD_DIM)
    mixed_input = lax.optimization_barrier((project(w_pre_gate) * project(w_conv_in)).astype(jnp.bfloat16)).astype(jnp.float32)
    padded = jnp.pad(mixed_input, ((1, 1), (0, 0)))
    tap_weights = conv_taps.astype(jnp.float32)
    convolved = tap_weights[0] * padded[:-2] + tap_weights[1] * padded[1:-1] + tap_weights[2] * padded[2:]
    conv_out = (project(w_post_gate) * convolved).astype(jnp.bfloat16)
    blocks = total_tokens // WINDOW
    group_size = HEADS // KV_HEADS
    pad_spec = ((WINDOW, WINDOW), (0, 0), (0, 0))
    keys_pad = jnp.pad(keys_rot, pad_spec)
    values_pad = jnp.pad(values_all, pad_spec)
    block_queries = queries.reshape(blocks, WINDOW, KV_HEADS, group_size, HEAD_DIM)
    sink_values = sink_logit.astype(jnp.float32).reshape(KV_HEADS, group_size)[:, :, None]

    def one_block(inputs):
        query_block, index = inputs
        key_block = lax.dynamic_slice_in_dim(keys_pad, index * WINDOW, 3 * WINDOW, 0)
        value_block = lax.dynamic_slice_in_dim(values_pad, index * WINDOW, 3 * WINDOW, 0)
        scores = jnp.einsum('qkgd,skd->kgqs', query_block.astype(jnp.float32), key_block.astype(jnp.float32)) * HEAD_DIM ** (-0.5)
        query_pos = index * WINDOW + jnp.arange(WINDOW, dtype=jnp.int32)
        key_pos = index * WINDOW - WINDOW + jnp.arange(3 * WINDOW, dtype=jnp.int32)
        allowed = (jnp.abs(key_pos[None, :] - query_pos[:, None]) <= WINDOW) & (key_pos >= 0)[None, :] & (key_pos < total_tokens)[None, :]
        scores = jnp.where(allowed[None, None], scores, -jnp.inf)
        row_max = jnp.maximum(lax.optimization_barrier(jnp.max(scores, axis=-1)), sink_values)
        exp_scores = jnp.exp(scores - row_max[..., None])
        denominator = lax.optimization_barrier(jnp.sum(exp_scores, axis=-1)) + jnp.exp(sink_values - row_max)
        weights = (exp_scores / denominator[..., None]).astype(jnp.bfloat16)
        attended = jnp.einsum('kgqs,skd->qkgd', weights.astype(jnp.float32), value_block.astype(jnp.float32)).astype(jnp.bfloat16)
        return (attended.reshape(WINDOW, HEADS * HEAD_DIM), row_max + jnp.log(denominator))
    attended, log_sum = lax.map(one_block, (block_queries, jnp.arange(blocks, dtype=jnp.int32)))
    attended = attended.reshape(total_tokens, HEADS * HEAD_DIM)
    log_weight_sum = jnp.transpose(log_sum, (1, 2, 0, 3)).reshape(HEADS, total_tokens)
    mixed = (jnp.dot(attended, w_out_attn, preferred_element_type=jnp.float32) + jnp.dot(conv_out, w_out_conv, preferred_element_type=jnp.float32)).astype(jnp.bfloat16)
    return (mixed, log_weight_sum)
```

```python
import functools

import jax
import jax.numpy as jnp
from jax import lax
from jax.experimental import pallas as pl
from jax.experimental.pallas import tpu as pltpu
from jax.sharding import PartitionSpec as P

MESH = pl.DeviceIdType.MESH

HEAD_DIM = 64
WINDOW = 128
GRID_W = 64


rope_base = 10000.0
norm_eps = 1e-06


def padded(block, sides, width):
    for axis, dim in sides:
        count = lax.axis_size(axis)
        forward = [(i, i + 1) for i in range(count - 1)]
        backward = [(target, source) for source, target in forward]
        low = lax.ppermute(
            lax.slice_in_dim(block, block.shape[dim] - width, None, axis=dim), axis, forward
        )
        high = lax.ppermute(lax.slice_in_dim(block, 0, width, axis=dim), axis, backward)
        block = jnp.concatenate([low, block, high], axis=dim)
    return block


def rotate_pair(values, angles):
    first_half, second_half = jnp.split(values, 2, axis=-1)
    cosine = jnp.cos(angles)[:, None, :]
    sine_part = jnp.sin(angles)[:, None, :]
    return jnp.concatenate(
        [
            first_half * cosine - second_half * sine_part,
            first_half * sine_part + second_half * cosine,
        ],
        axis=-1,
    )


def axial_rotate(values, positions):
    half_dim = values.shape[-1] // 2
    inv_freq = rope_base ** (-jnp.arange(0, half_dim, 2).astype(jnp.float32) / half_dim)
    row_angle = (positions // GRID_W).astype(jnp.float32)[:, None] * inv_freq
    col_angle = (positions % GRID_W).astype(jnp.float32)[:, None] * inv_freq
    row_part, col_part = jnp.split(values, 2, axis=-1)
    return jnp.concatenate(
        [rotate_pair(row_part, row_angle), rotate_pair(col_part, col_angle)], axis=-1
    )


def block_windows(source, rows_local, blocks):
    pieces = [
        source[step * WINDOW : step * WINDOW + rows_local].reshape(
            (blocks, WINDOW) + source.shape[1:]
        )
        for step in range(3)
    ]
    return jnp.concatenate(pieces, axis=1)


def on_device(
    tokens,
    norm_gain,
    w_query,
    w_key,
    w_value,
    w_post_gate,
    w_pre_gate,
    w_conv_in,
    conv_taps,
    sink_logit,
    w_out_attn,
    w_out_conv,
):
    whole = lax.all_gather(tokens, "tp", axis=1, tiled=True)
    rows_local = whole.shape[0]
    whole_float = whole.astype(jnp.float32)
    mean_square = jnp.mean(whole_float * whole_float, axis=1, keepdims=True)
    normed = (whole_float * lax.rsqrt(mean_square + norm_eps) * norm_gain).astype(jnp.bfloat16)
    col_widths = [
        w_query.shape[1],
        w_key.shape[1],
        w_value.shape[1],
        w_post_gate.shape[1],
        w_pre_gate.shape[1],
        w_conv_in.shape[1],
    ]
    joined = jnp.concatenate(
        (
            lax.all_gather(w_query, "sp", axis=0, tiled=True),
            lax.all_gather(w_key, "sp", axis=0, tiled=True),
            lax.all_gather(w_value, "sp", axis=0, tiled=True),
            lax.all_gather(w_post_gate, "sp", axis=0, tiled=True),
            lax.all_gather(w_pre_gate, "sp", axis=0, tiled=True),
            lax.all_gather(w_conv_in, "sp", axis=0, tiled=True),
        ),
        axis=1,
    )
    projected = jnp.dot(normed, joined, preferred_element_type=jnp.float32)
    bounds = []
    running = 0
    for col_width in col_widths[:-1]:
        running += col_width
        bounds.append(running)
    query_raw, key_raw, value_raw, post_gate, pre_gate, conv_input = jnp.split(
        projected, bounds, axis=1
    )
    offset = lax.axis_index("sp") * rows_local
    positions = offset + jnp.arange(rows_local, dtype=jnp.int32)
    local_heads = w_query.shape[1] // HEAD_DIM
    local_groups = w_key.shape[1] // HEAD_DIM
    group_size = local_heads // local_groups
    queries = axial_rotate(query_raw.reshape(rows_local, local_heads, HEAD_DIM), positions).astype(
        jnp.bfloat16
    )
    keys_rot = axial_rotate(key_raw.reshape(rows_local, local_groups, HEAD_DIM), positions).astype(
        jnp.bfloat16
    )
    key_value = jnp.concatenate(
        [keys_rot.reshape(rows_local, local_groups * HEAD_DIM), value_raw.astype(jnp.bfloat16)],
        axis=1,
    )
    mixed_input = (pre_gate * conv_input).astype(jnp.bfloat16)
    kv_padded = padded(key_value, (("sp", 0),), WINDOW)
    conv_padded = padded(mixed_input, (("sp", 0),), 1)
    conv_float = conv_padded.astype(jnp.float32)
    convolved = (
        conv_taps[0] * conv_float[:-2]
        + conv_taps[1] * conv_float[1:-1]
        + conv_taps[2] * conv_float[2:]
    )
    conv_out = (post_gate * convolved).astype(jnp.bfloat16)
    total_tokens = rows_local * lax.axis_size("sp")
    blocks = rows_local // WINDOW
    padded_rows = rows_local + 2 * WINDOW
    block_queries = queries.reshape(blocks, WINDOW, local_groups, group_size, HEAD_DIM)
    block_keys = block_windows(
        kv_padded[:, : local_groups * HEAD_DIM].reshape(padded_rows, local_groups, HEAD_DIM),
        rows_local,
        blocks,
    )
    block_values = block_windows(
        kv_padded[:, local_groups * HEAD_DIM :].reshape(padded_rows, local_groups, HEAD_DIM),
        rows_local,
        blocks,
    )
    scores = jnp.einsum(
        "nqkgd,nskd->nkgqs", block_queries, block_keys, preferred_element_type=jnp.float32
    ) * HEAD_DIM ** (-0.5)
    query_pos = positions.reshape(blocks, WINDOW)
    key_pos = (
        offset
        - WINDOW
        + (jnp.arange(blocks, dtype=jnp.int32) * WINDOW)[:, None]
        + jnp.arange(3 * WINDOW, dtype=jnp.int32)[None, :]
    )
    distance = key_pos[:, None, :] - query_pos[:, :, None]
    allowed = (
        (jnp.abs(distance) <= WINDOW)
        & (key_pos >= 0)[:, None, :]
        & (key_pos < total_tokens)[:, None, :]
    )
    scores = jnp.where(allowed[:, None, None], scores, -jnp.inf)
    sink_values = sink_logit.reshape(local_groups, group_size)[None, :, :, None]
    row_max = jnp.maximum(jnp.max(scores, axis=-1), sink_values)
    exp_scores = jnp.exp(scores - row_max[..., None])
    denominator = jnp.sum(exp_scores, axis=-1) + jnp.exp(sink_values - row_max)
    weights = (exp_scores / denominator[..., None]).astype(jnp.bfloat16)
    attended = (
        jnp.einsum("nkgqs,nskd->nqkgd", weights, block_values, preferred_element_type=jnp.float32)
        .astype(jnp.bfloat16)
        .reshape(rows_local, local_heads * HEAD_DIM)
    )
    log_sum = row_max + jnp.log(denominator)
    log_weight_sum = jnp.transpose(log_sum, (1, 2, 0, 3)).reshape(local_heads, rows_local)
    out_attn, out_conv = (
        lax.all_gather(w_out_attn, "sp", axis=1, tiled=True),
        lax.all_gather(w_out_conv, "sp", axis=1, tiled=True),
    )
    mixed = lax.psum_scatter(
        (
            jnp.dot(attended, out_attn, preferred_element_type=jnp.float32)
            + jnp.dot(conv_out, out_conv, preferred_element_type=jnp.float32)
        ).astype(jnp.bfloat16),
        "tp",
        scatter_dimension=0,
        tiled=True,
    )
    return (mixed, log_weight_sum)


def rope_tables(rows, lanes):
    half_dim = HEAD_DIM // 2
    positions = lax.axis_index("sp") * rows + jnp.arange(rows, dtype=jnp.int32)
    lane = jnp.arange(lanes, dtype=jnp.int32) % HEAD_DIM
    freq_index = lane % (half_dim // 2)
    inv_freq = rope_base ** (-(2 * freq_index).astype(jnp.float32) / half_dim)
    is_col = lane >= half_dim
    index = jnp.where(is_col[None, :], (positions % GRID_W)[:, None], (positions // GRID_W)[:, None])
    angle = index.astype(jnp.float32) * inv_freq[None, :]
    sign = jnp.where((lane % half_dim) < half_dim // 2, -1.0, 1.0)
    return jnp.cos(angle), jnp.sin(angle) * sign[None, :]


def fused_kernel(
    Z, X,
    tok_ref, gain_ref, win_ref, oa_ref, oc_ref, cos_ref, sin_ref, taps_ref, sink_ref,
    out_ref, lse_ref,
    tok, normed, win, woa, woc, acc, qbuf, kvp, cf, chalo_out, chalo_in, att, cout,
    part_keep, part_send, part_recv, y_send, y_recv,
    tok_sem, in_send, in_recv, oa_send, oa_recv, oc_send, oc_recv, halo_sem, rs_sem, loc_sem,
):
    S = Z * X
    rows, width = tok_ref.shape
    depth = win_ref.shape[0]
    cols = oa_ref.shape[1]
    qw = qbuf.shape[1]
    cw = cf.shape[1]
    sp = lax.axis_index("sp")
    tp = lax.axis_index("tp")
    z, x = sp // X, sp % X
    core, yy = tp % 2, tp // 2
    sib = tp + 1 - 2 * core
    ynb = (1 - yy) * 2 + core
    ysib = (1 - yy) * 2 + 1 - core
    xnb = z * X + 1 - x
    low, high = sp - X, sp + X
    has_low, has_high = z > 0, z < Z - 1
    has_prev, has_next = sp > 0, sp < S - 1

    barrier = pltpu.get_barrier_semaphore()

    def greet(dev):
        pl.semaphore_signal(barrier, inc=1, device_id=dev, device_id_type=MESH)

    greet((xnb, tp))
    greet((sp, sib))
    greet((sp, ynb))
    for cond, dev in ((has_low, low), (has_high, high), (has_prev, sp - 1), (has_next, sp + 1)):
        @pl.when(cond)
        def _(dev=dev):
            greet((dev, tp))
    peers = 3
    for cond in (has_low, has_high, has_prev, has_next):
        peers = peers + jnp.where(cond, 1, 0)
    pl.semaphore_wait(barrier, peers)

    def remote(src, dst, ssem, rsem, dev):
        return pltpu.make_async_remote_copy(
            src_ref=src, dst_ref=dst, send_sem=ssem, recv_sem=rsem,
            device_id=dev, device_id_type=MESH,
        )

    targets = (low, high, xnb)

    def weight_copy(kind, slot, direction, own=False):
        buf, ssem, rsem, ref = (
            (win, in_send, in_recv, win_ref),
            (woa, oa_send, oa_recv, oa_ref),
            (woc, oc_send, oc_recv, oc_ref),
        )[kind]
        source = ref if own else buf.at[slot]
        return remote(source, buf.at[slot], ssem.at[direction, slot], rsem.at[slot], (targets[direction], tp))

    weight_copy(2, sp, 2, True).start()
    @pl.when(has_low)
    def _():
        weight_copy(0, sp, 0, True).start()
    @pl.when(has_high)
    def _():
        weight_copy(0, sp, 1, True).start()
    weight_copy(0, sp, 2, True).start()

    tok_y = remote(tok_ref, tok.at[tp], tok_sem.at[0], tok_sem.at[1], (sp, ynb))
    tok_y.start()
    tok_s = remote(tok_ref, tok.at[tp], tok_sem.at[2], tok_sem.at[3], (sp, sib))
    tok_s.start()
    local = [
        pltpu.make_async_copy(tok_ref, tok.at[tp], loc_sem.at[0]),
        pltpu.make_async_copy(win_ref, win.at[sp], loc_sem.at[1]),
        pltpu.make_async_copy(oa_ref, woa.at[sp], loc_sem.at[2]),
        pltpu.make_async_copy(oc_ref, woc.at[sp], loc_sem.at[3]),
    ]
    for copy in local:
        copy.start()
    for copy in local:
        copy.wait()
    remote(tok.at[ynb], tok.at[ynb], tok_sem.at[0], tok_sem.at[1], (sp, ynb)).wait_recv()
    tok_f = remote(tok.at[ynb], tok.at[ynb], tok_sem.at[4], tok_sem.at[5], (sp, sib))
    tok_f.start()
    remote(tok.at[sib], tok.at[sib], tok_sem.at[2], tok_sem.at[3], (sp, sib)).wait_recv()
    remote(tok.at[ysib], tok.at[ysib], tok_sem.at[4], tok_sem.at[5], (sp, sib)).wait_recv()

    TP = tok.shape[0]
    RB = 64

    def norm_rows(i, carry):
        r = pl.ds(pl.multiple_of(i * RB, RB), RB)
        total = jnp.zeros((RB, 1), jnp.float32)
        for t in range(TP):
            v = tok[t, r, :].astype(jnp.float32)
            total += jnp.sum(v * v, axis=1, keepdims=True)
        scale = lax.rsqrt(total / (TP * width) + norm_eps)
        for t in range(TP):
            v = tok[t, r, :].astype(jnp.float32)
            g = gain_ref[:, t * width:(t + 1) * width]
            normed[r, t * width:(t + 1) * width] = (v * scale * g).astype(jnp.bfloat16)
        return carry

    lax.fori_loop(0, rows // RB, norm_rows, 0)

    MB = 128

    def project(slot, first):
        def body(i, carry):
            r = pl.ds(pl.multiple_of(i * MB, MB), MB)
            c = pl.ds(pl.multiple_of(slot * depth, depth), depth)
            prod = jnp.dot(normed[r, c], win[slot], preferred_element_type=jnp.float32)
            if first:
                acc[r, :] = prod
            else:
                acc[r, :] += prod
            return carry
        lax.fori_loop(0, rows // MB, body, 0)

    def entry(k):
        dist = (k + 1) // 2
        up = 1 - k % 2
        zz = z + dist * (2 * up - 1)
        return zz, up, (zz >= 0) & (zz < Z)

    def wait_weight(kind, slot):
        weight_copy(kind, slot, 2).wait_recv()

    def pass_on(kind, slot, up, across):
        @pl.when((up == 1) & has_low)
        def _():
            weight_copy(kind, slot, 0).start()
        @pl.when((up == 0) & has_high)
        def _():
            weight_copy(kind, slot, 1).start()
        if across:
            weight_copy(kind, slot, 2).start()

    entries = 2 * Z - 1

    def start_out_weights():
        for direction, cond in ((0, has_low), (1, has_high)):
            @pl.when(cond)
            def _(direction=direction):
                weight_copy(1, sp, direction, True).start()
                weight_copy(2, sp, direction, True).start()
        weight_copy(1, sp, 2, True).start()
        wait_weight(2, xnb)
        for direction, cond in ((0, has_low), (1, has_high)):
            @pl.when(cond)
            def _(direction=direction):
                weight_copy(2, xnb, direction).start()

    project(sp, True)

    def in_step(k, carry):
        zz, up, valid = entry(k)

        @pl.when(valid & (k < entries))
        def _():
            slot = zz * X + x
            wait_weight(0, slot)
            pass_on(0, slot, up, True)
            project(slot, False)

        @pl.when(k == 2 * (Z - 2))
        def _():
            start_out_weights()

        zo, _, valid_o = entry(k - 2)

        @pl.when(valid_o & (k >= 2))
        def _():
            slot = zo * X + 1 - x
            wait_weight(0, slot)
            project(slot, False)
        return carry

    lax.fori_loop(1, entries + 2, in_step, 0)

    def out_comm(dist):
        for up in (0, 1):
            zz = z + dist * (2 * up - 1)

            @pl.when((zz >= 0) & (zz < Z))
            def _(zz=zz, up=up):
                mine, other = zz * X + x, zz * X + 1 - x
                wait_weight(1, mine)
                pass_on(1, mine, up, True)
                wait_weight(2, mine)
                pass_on(2, mine, up, False)
                wait_weight(2, other)
                pass_on(2, other, up, False)

    def turned(v, cosv, sinv):
        lane = lax.broadcasted_iota(jnp.int32, v.shape, 1)
        quarter = HEAD_DIM // 4
        partner = jnp.where(
            lane % (2 * quarter) < quarter,
            pltpu.roll(v, v.shape[1] - quarter, 1),
            pltpu.roll(v, quarter, 1),
        )
        return v * cosv + partner * sinv

    kw = 2 * HEAD_DIM

    def kv_rows(i, carry):
        r = pl.ds(pl.multiple_of(i * MB, MB), MB)
        v = acc[r, qw:qw + kw]
        lane = lax.broadcasted_iota(jnp.int32, v.shape, 1)
        kv = jnp.where(lane < HEAD_DIM, turned(v, cos_ref[r, :], sin_ref[r, :]), v)
        kvp[pl.ds(pl.multiple_of(WINDOW + i * MB, MB), MB), :] = kv.astype(jnp.bfloat16)
        base = qw + kw + cw
        mi = (acc[r, base:base + cw] * acc[r, base + cw:base + 2 * cw]).astype(jnp.bfloat16)
        cf[pl.ds(pl.multiple_of(8 + i * MB, 8), MB), :] = mi.astype(jnp.float32)
        return carry

    lax.fori_loop(0, rows // MB, kv_rows, 0)
    E = chalo_out.shape[1]
    chalo_out[0] = cf[8:8 + E, :].astype(jnp.bfloat16)
    chalo_out[1] = cf[8 + rows - E:8 + rows, :].astype(jnp.bfloat16)

    to_next = [
        remote(kvp.at[pl.ds(rows, WINDOW)], kvp.at[pl.ds(0, WINDOW)], halo_sem.at[0], halo_sem.at[1], (sp + 1, tp)),
        remote(chalo_out.at[1], chalo_in.at[0], halo_sem.at[2], halo_sem.at[3], (sp + 1, tp)),
    ]
    to_prev = [
        remote(kvp.at[pl.ds(WINDOW, WINDOW)], kvp.at[pl.ds(WINDOW + rows, WINDOW)], halo_sem.at[4], halo_sem.at[5], (sp - 1, tp)),
        remote(chalo_out.at[0], chalo_in.at[1], halo_sem.at[6], halo_sem.at[7], (sp - 1, tp)),
    ]

    @pl.when(has_next)
    def _():
        for copy in to_next:
            copy.start()

    @pl.when(has_prev)
    def _():
        for copy in to_prev:
            copy.start()

    out_comm(1)

    def q_rows(i, carry):
        r = pl.ds(pl.multiple_of(i * MB, MB), MB)
        for c in range(qw // kw):
            qbuf[r, c * kw:(c + 1) * kw] = turned(
                acc[r, c * kw:(c + 1) * kw], cos_ref[r, :], sin_ref[r, :]
            ).astype(jnp.bfloat16)
        return carry

    lax.fori_loop(0, rows // MB, q_rows, 0)

    zero_kv = jnp.zeros((WINDOW, kw), jnp.bfloat16)
    zero_c = jnp.zeros((8, cw), jnp.float32)

    @pl.when(has_prev)
    def _():
        for copy in to_next:
            copy.wait_recv()
        cf[0:8, :] = chalo_in[0, E - 8:E, :].astype(jnp.float32)

    @pl.when(jnp.logical_not(has_prev))
    def _():
        kvp[0:WINDOW, :] = zero_kv
        cf[0:8, :] = zero_c

    @pl.when(has_next)
    def _():
        for copy in to_prev:
            copy.wait_recv()
        cf[8 + rows:16 + rows, :] = chalo_in[1, 0:8, :].astype(jnp.float32)

    @pl.when(jnp.logical_not(has_next))
    def _():
        kvp[WINDOW + rows:, :] = zero_kv
        cf[8 + rows:16 + rows, :] = zero_c

    taps = [taps_ref[t:t + 1, :] for t in range(3)]
    for i in range(rows // MB):
        a = 8 + i * MB
        conv = (
            taps[0] * cf[a - 1:a - 1 + MB, :]
            + taps[1] * cf[a:a + MB, :]
            + taps[2] * cf[a + 1:a + 1 + MB, :]
        )
        cout[i * MB:(i + 1) * MB, :] = (acc[i * MB:(i + 1) * MB, qw + kw:qw + kw + cw] * conv).astype(jnp.bfloat16)

    heads = qw // HEAD_DIM
    K3 = 3 * WINDOW
    total_tokens = rows * S

    def attend(b, carry):
        r = pl.ds(pl.multiple_of(b * WINDOW, WINDOW), WINDOW)
        kv = kvp[pl.ds(pl.multiple_of(b * WINDOW, WINDOW), K3), :].astype(jnp.float32)
        lane = lax.broadcasted_iota(jnp.int32, (K3, kw), 1)
        swapped = pltpu.roll(kv, HEAD_DIM, 1)
        kk = jnp.where(lane < HEAD_DIM, kv, swapped).astype(jnp.bfloat16)
        vv = jnp.where(lane < HEAD_DIM, swapped, kv).astype(jnp.bfloat16)
        k_half = [jnp.where(lane < HEAD_DIM, kk, 0), jnp.where(lane < HEAD_DIM, 0, kk)]
        v_half = [jnp.where(lane < HEAD_DIM, vv, 0), jnp.where(lane < HEAD_DIM, 0, vv)]
        qi = lax.broadcasted_iota(jnp.int32, (WINDOW, K3), 0)
        ki = lax.broadcasted_iota(jnp.int32, (WINDOW, K3), 1)
        first = sp * rows + b * WINDOW - WINDOW
        allowed = (ki >= qi) & (ki <= qi + 2 * WINDOW) & (ki + first >= 0) & (ki + first < total_tokens)
        lse_lane = lax.broadcasted_iota(jnp.int32, (WINDOW, WINDOW), 1)
        lse_all = jnp.zeros((WINDOW, WINDOW), jnp.float32)
        for pair in range(heads // 2):
            q = qbuf[r, pair * kw:(pair + 1) * kw]
            total = jnp.zeros((WINDOW, kw), jnp.float32)
            for side in range(2):
                h = pair * 2 + side
                s = lax.dot_general(
                    q, k_half[side], (((1,), (1,)), ((), ())), preferred_element_type=jnp.float32
                ) * HEAD_DIM ** (-0.5)
                s = jnp.where(allowed, s, -jnp.inf)
                sink = sink_ref[h:h + 1, 0:1]
                top = jnp.maximum(jnp.max(s, axis=1, keepdims=True), sink)
                e = jnp.exp(s - top)
                den = jnp.sum(e, axis=1, keepdims=True) + jnp.exp(sink - top)
                w = (e * (1.0 / den)).astype(jnp.bfloat16)
                total += jnp.dot(w, v_half[side], preferred_element_type=jnp.float32)
                lse_all = jnp.where(lse_lane == h, top + jnp.log(den), lse_all)
            att[r, pair * kw:(pair + 1) * kw] = total.astype(jnp.bfloat16)
        lse_ref[:, r] = jnp.transpose(lse_all)[0:heads, :]
        return carry

    blocks = rows // WINDOW
    lax.fori_loop(0, blocks // 2, attend, 0)
    if Z > 2:
        out_comm(2)
    lax.fori_loop(blocks // 2, blocks, attend, 0)
    for dist in range(3, Z):
        out_comm(dist)

    chunk = rows // TP

    def sib_copy(slot):
        return remote(part_send.at[slot], part_recv.at[slot], rs_sem.at[0, slot], rs_sem.at[1, slot], (sp, sib))

    def y_copy(slot):
        return remote(y_send.at[slot], y_recv.at[slot], rs_sem.at[2, slot], rs_sem.at[3, slot], (sp, ynb))

    def out_block(slot):
        for half in range(2):
            for mine in range(2):
                t = half * 2 + (core if mine else 1 - core)
                r = pl.ds(pl.multiple_of(t * chunk, chunk), chunk)
                v = jnp.dot(att[r, :], woa[slot], preferred_element_type=jnp.float32) + jnp.dot(
                    cout[r, :], woc[slot], preferred_element_type=jnp.float32
                )
                if mine:
                    part_keep[slot, half] = v
                else:
                    part_send[slot, half] = v.astype(jnp.bfloat16)
        sib_copy(slot).start()

    def y_block(slot):
        sib_copy(slot).wait_recv()
        y_send[slot] = (
            part_keep[slot, 1 - yy] + part_recv[slot, 1 - yy].astype(jnp.float32)
        ).astype(jnp.bfloat16)
        y_copy(slot).start()

    def finish(slot):
        y_copy(slot).wait_recv()
        out_ref[:, pl.ds(pl.multiple_of(slot * cols, cols), cols)] = (
            part_keep[slot, yy]
            + part_recv[slot, yy].astype(jnp.float32)
            + y_recv[slot].astype(jnp.float32)
        ).astype(jnp.bfloat16)

    def each(fn, lo, hi):
        def step(u, carry):
            k, side = u // 2, u % 2
            zz, _, valid = entry(k)

            @pl.when(valid)
            def _():
                slot = zz * X + jnp.where(side == 0, x, 1 - x)
                fn(slot, k, side)
            return carry
        lax.fori_loop(lo, hi, step, 0)

    def project_out(slot, k, side):
        @pl.when(side == 1)
        def _():
            wait_weight(1, slot)
        out_block(slot)

    half_u = entries
    each(project_out, 0, half_u)
    each(lambda slot, k, side: y_block(slot), 0, half_u)
    each(project_out, half_u, 2 * entries)
    each(lambda slot, k, side: y_block(slot), half_u, 2 * entries)
    each(lambda slot, k, side: finish(slot), 0, 2 * entries)

    tok_y.wait_send()
    tok_s.wait_send()
    tok_f.wait_send()

    @pl.when(has_next)
    def _():
        for copy in to_next:
            copy.wait_send()

    @pl.when(has_prev)
    def _():
        for copy in to_prev:
            copy.wait_send()

    def drain(zz, carry):
        mine, other = zz * X + x, zz * X + 1 - x
        for direction, cond in ((0, (zz >= z) & has_low), (1, (zz <= z) & has_high)):
            @pl.when(cond)
            def _(direction=direction):
                weight_copy(0, mine, direction).wait_send()
                weight_copy(1, mine, direction).wait_send()
                weight_copy(2, mine, direction).wait_send()
                weight_copy(2, other, direction).wait_send()
        weight_copy(0, mine, 2).wait_send()
        weight_copy(1, mine, 2).wait_send()
        for slot in (mine, other):
            sib_copy(slot).wait_send()
            y_copy(slot).wait_send()
        return carry

    lax.fori_loop(0, Z, drain, 0)
    weight_copy(2, sp, 2).wait_send()


def fused(
    tokens, norm_gain, w_query, w_key, w_value, w_post_gate, w_pre_gate, w_conv_in,
    conv_taps, sink_logit, w_out_attn, w_out_conv,
):
    S, TP = lax.axis_size("sp"), lax.axis_size("tp")
    X = 2
    Z = S // X
    rows, width = tokens.shape
    depth, qw = w_query.shape
    cw = w_post_gate.shape[1]
    cols = w_out_attn.shape[1]
    heads = qw // HEAD_DIM
    kw = 2 * HEAD_DIM
    joined = jnp.concatenate((w_query, w_key, w_value, w_post_gate, w_pre_gate, w_conv_in), axis=1)
    nw = joined.shape[1]
    cosv, sinv = rope_tables(rows, kw)
    chunk = rows // TP
    bf, f32 = jnp.bfloat16, jnp.float32
    dma = pltpu.SemaphoreType.DMA
    sinks = jnp.broadcast_to(sink_logit[:, None], (heads, kw))
    return pl.pallas_call(
        functools.partial(fused_kernel, Z, X),
        out_shape=(
            jax.ShapeDtypeStruct((chunk, S * cols), bf),
            jax.ShapeDtypeStruct((heads, rows), f32),
        ),
        in_specs=[pl.BlockSpec(memory_space=pltpu.VMEM)] * 9,
        out_specs=(pl.BlockSpec(memory_space=pltpu.VMEM),) * 2,
        scratch_shapes=[
            pltpu.VMEM((TP, rows, width), bf),
            pltpu.VMEM((rows, TP * width), bf),
            pltpu.VMEM((S, depth, nw), bf),
            pltpu.VMEM((S,) + w_out_attn.shape, bf),
            pltpu.VMEM((S,) + w_out_conv.shape, bf),
            pltpu.VMEM((rows, nw), f32),
            pltpu.VMEM((rows, qw), bf),
            pltpu.VMEM((rows + 2 * WINDOW, kw), bf),
            pltpu.VMEM((rows + 16, cw), f32),
            pltpu.VMEM((2, 16, cw), bf),
            pltpu.VMEM((2, 16, cw), bf),
            pltpu.VMEM((rows, qw), bf),
            pltpu.VMEM((rows, cw), bf),
            pltpu.VMEM((S, 2, chunk, cols), f32),
            pltpu.VMEM((S, 2, chunk, cols), bf),
            pltpu.VMEM((S, 2, chunk, cols), bf),
            pltpu.VMEM((S, chunk, cols), bf),
            pltpu.VMEM((S, chunk, cols), bf),
            dma((6,)),
            dma((3, S)), dma((S,)),
            dma((3, S)), dma((S,)),
            dma((3, S)), dma((S,)),
            dma((8,)),
            dma((4, S)),
            dma((4,)),
        ],
        compiler_params=pltpu.CompilerParams(
            collective_id=0, has_side_effects=True, vmem_limit_bytes=60 * 1024 * 1024
        ),
    )(tokens, norm_gain[None, :], joined, w_out_attn, w_out_conv, cosv, sinv, conv_taps, sinks)


def fits(
    tokens, norm_gain, w_query, w_key, w_value, w_post_gate, w_pre_gate, w_conv_in,
    conv_taps, sink_logit, w_out_attn, w_out_conv,
):
    S, TP = lax.axis_size("sp"), lax.axis_size("tp")
    return (
        TP == 4
        and S % 2 == 0
        and S >= 4
        and w_key.shape[1] == HEAD_DIM
        and w_query.shape[0] % 128 == 0
        and w_query.shape[1] % 128 == 0
        and w_post_gate.shape[1] % 128 == 0
        and w_out_attn.shape[1] % 128 == 0
        and tokens.shape[0] % (TP * WINDOW) == 0
        and tokens.shape[1] % 128 == 0
    )


def either(*args):
    return fused(*args) if fits(*args) else on_device(*args)


def solution(mesh):
    placed = (
        P("sp", "tp"),
        P(),
        P("sp", "tp"),
        P("sp", "tp"),
        P("sp", "tp"),
        P("sp", "tp"),
        P("sp", "tp"),
        P("sp", "tp"),
        P(None, "tp"),
        P("tp"),
        P("tp", "sp"),
        P("tp", "sp"),
    )
    return jax.shard_map(
        either,
        mesh=mesh,
        in_specs=placed,
        out_specs=(P(("sp", "tp"), None), P("tp", "sp")),
        check_vma=False,
    )
```

```python
import functools
import math

import jax
import jax.numpy as jnp
from jax import lax
from jax.experimental import pallas as pl
from jax.experimental.pallas import tpu as pltpu
from jax.sharding import PartitionSpec as P

MESH = pl.DeviceIdType.MESH

HEAD_DIM = 64
WINDOW = 128
GRID_W = 64


rope_base = 10000.0
norm_eps = 1e-06


def padded(block, sides, width):
    for axis, dim in sides:
        count = lax.axis_size(axis)
        forward = [(i, i + 1) for i in range(count - 1)]
        backward = [(target, source) for source, target in forward]
        low = lax.ppermute(
            lax.slice_in_dim(block, block.shape[dim] - width, None, axis=dim), axis, forward
        )
        high = lax.ppermute(lax.slice_in_dim(block, 0, width, axis=dim), axis, backward)
        block = jnp.concatenate([low, block, high], axis=dim)
    return block


def rotate_pair(values, angles):
    first_half, second_half = jnp.split(values, 2, axis=-1)
    cosine = jnp.cos(angles)[:, None, :]
    sine_part = jnp.sin(angles)[:, None, :]
    return jnp.concatenate(
        [
            first_half * cosine - second_half * sine_part,
            first_half * sine_part + second_half * cosine,
        ],
        axis=-1,
    )


def axial_rotate(values, positions):
    half_dim = values.shape[-1] // 2
    inv_freq = rope_base ** (-jnp.arange(0, half_dim, 2).astype(jnp.float32) / half_dim)
    row_angle = (positions // GRID_W).astype(jnp.float32)[:, None] * inv_freq
    col_angle = (positions % GRID_W).astype(jnp.float32)[:, None] * inv_freq
    row_part, col_part = jnp.split(values, 2, axis=-1)
    return jnp.concatenate(
        [rotate_pair(row_part, row_angle), rotate_pair(col_part, col_angle)], axis=-1
    )


def block_windows(source, rows_local, blocks):
    pieces = [
        source[step * WINDOW : step * WINDOW + rows_local].reshape(
            (blocks, WINDOW) + source.shape[1:]
        )
        for step in range(3)
    ]
    return jnp.concatenate(pieces, axis=1)


def on_device(
    tokens,
    norm_gain,
    w_query,
    w_key,
    w_value,
    w_post_gate,
    w_pre_gate,
    w_conv_in,
    conv_taps,
    sink_logit,
    w_out_attn,
    w_out_conv,
):
    whole = lax.all_gather(tokens, "tp", axis=1, tiled=True)
    rows_local = whole.shape[0]
    whole_float = whole.astype(jnp.float32)
    mean_square = jnp.mean(whole_float * whole_float, axis=1, keepdims=True)
    normed = (whole_float * lax.rsqrt(mean_square + norm_eps) * norm_gain).astype(jnp.bfloat16)
    col_widths = [
        w_query.shape[1],
        w_key.shape[1],
        w_value.shape[1],
        w_post_gate.shape[1],
        w_pre_gate.shape[1],
        w_conv_in.shape[1],
    ]
    joined = jnp.concatenate(
        (
            lax.all_gather(w_query, "sp", axis=0, tiled=True),
            lax.all_gather(w_key, "sp", axis=0, tiled=True),
            lax.all_gather(w_value, "sp", axis=0, tiled=True),
            lax.all_gather(w_post_gate, "sp", axis=0, tiled=True),
            lax.all_gather(w_pre_gate, "sp", axis=0, tiled=True),
            lax.all_gather(w_conv_in, "sp", axis=0, tiled=True),
        ),
        axis=1,
    )
    projected = jnp.dot(normed, joined, preferred_element_type=jnp.float32)
    bounds = []
    running = 0
    for col_width in col_widths[:-1]:
        running += col_width
        bounds.append(running)
    query_raw, key_raw, value_raw, post_gate, pre_gate, conv_input = jnp.split(
        projected, bounds, axis=1
    )
    offset = lax.axis_index("sp") * rows_local
    positions = offset + jnp.arange(rows_local, dtype=jnp.int32)
    local_heads = w_query.shape[1] // HEAD_DIM
    local_groups = w_key.shape[1] // HEAD_DIM
    group_size = local_heads // local_groups
    queries = axial_rotate(query_raw.reshape(rows_local, local_heads, HEAD_DIM), positions).astype(
        jnp.bfloat16
    )
    keys_rot = axial_rotate(key_raw.reshape(rows_local, local_groups, HEAD_DIM), positions).astype(
        jnp.bfloat16
    )
    key_value = jnp.concatenate(
        [keys_rot.reshape(rows_local, local_groups * HEAD_DIM), value_raw.astype(jnp.bfloat16)],
        axis=1,
    )
    mixed_input = (pre_gate * conv_input).astype(jnp.bfloat16)
    kv_padded = padded(key_value, (("sp", 0),), WINDOW)
    conv_padded = padded(mixed_input, (("sp", 0),), 1)
    conv_float = conv_padded.astype(jnp.float32)
    convolved = (
        conv_taps[0] * conv_float[:-2]
        + conv_taps[1] * conv_float[1:-1]
        + conv_taps[2] * conv_float[2:]
    )
    conv_out = (post_gate * convolved).astype(jnp.bfloat16)
    total_tokens = rows_local * lax.axis_size("sp")
    blocks = rows_local // WINDOW
    padded_rows = rows_local + 2 * WINDOW
    block_queries = queries.reshape(blocks, WINDOW, local_groups, group_size, HEAD_DIM)
    block_keys = block_windows(
        kv_padded[:, : local_groups * HEAD_DIM].reshape(padded_rows, local_groups, HEAD_DIM),
        rows_local,
        blocks,
    )
    block_values = block_windows(
        kv_padded[:, local_groups * HEAD_DIM :].reshape(padded_rows, local_groups, HEAD_DIM),
        rows_local,
        blocks,
    )
    scores = jnp.einsum(
        "nqkgd,nskd->nkgqs", block_queries, block_keys, preferred_element_type=jnp.float32
    ) * HEAD_DIM ** (-0.5)
    query_pos = positions.reshape(blocks, WINDOW)
    key_pos = (
        offset
        - WINDOW
        + (jnp.arange(blocks, dtype=jnp.int32) * WINDOW)[:, None]
        + jnp.arange(3 * WINDOW, dtype=jnp.int32)[None, :]
    )
    distance = key_pos[:, None, :] - query_pos[:, :, None]
    allowed = (
        (jnp.abs(distance) <= WINDOW)
        & (key_pos >= 0)[:, None, :]
        & (key_pos < total_tokens)[:, None, :]
    )
    scores = jnp.where(allowed[:, None, None], scores, -jnp.inf)
    sink_values = sink_logit.reshape(local_groups, group_size)[None, :, :, None]
    row_max = jnp.maximum(jnp.max(scores, axis=-1), sink_values)
    exp_scores = jnp.exp(scores - row_max[..., None])
    denominator = jnp.sum(exp_scores, axis=-1) + jnp.exp(sink_values - row_max)
    weights = (exp_scores / denominator[..., None]).astype(jnp.bfloat16)
    attended = (
        jnp.einsum("nkgqs,nskd->nqkgd", weights, block_values, preferred_element_type=jnp.float32)
        .astype(jnp.bfloat16)
        .reshape(rows_local, local_heads * HEAD_DIM)
    )
    log_sum = row_max + jnp.log(denominator)
    log_weight_sum = jnp.transpose(log_sum, (1, 2, 0, 3)).reshape(local_heads, rows_local)
    out_attn, out_conv = (
        lax.all_gather(w_out_attn, "sp", axis=1, tiled=True),
        lax.all_gather(w_out_conv, "sp", axis=1, tiled=True),
    )
    mixed = lax.psum_scatter(
        (
            jnp.dot(attended, out_attn, preferred_element_type=jnp.float32)
            + jnp.dot(conv_out, out_conv, preferred_element_type=jnp.float32)
        ).astype(jnp.bfloat16),
        "tp",
        scatter_dimension=0,
        tiled=True,
    )
    return (mixed, log_weight_sum)


def fused_kernel(
    Z, X,
    tok_ref, gain_ref, wq_ref, wk_ref, wv_ref, wpost_ref, wpre_ref, wcin_ref, oa_ref, oc_ref, taps_ref, sink_ref,
    out_ref, lse_ref,
    cos_ref, sin_ref, tok, normed, win, woa, woc, acc, qbuf, kvp, cf, chalo_out, chalo_in, att, cout,
    part_keep, part_send, part_recv, y_send, y_recv,
    tok_sem, in_send, in_recv, oa_send, oa_recv, oc_send, oc_recv, halo_sem, rs_sem, loc_sem,
):
    S = Z * X
    rows, width = tok_ref.shape
    depth = wq_ref.shape[0]
    piece = depth // 2
    cols = oa_ref.shape[1]
    qw = qbuf.shape[1]
    cw = cf.shape[1]
    sp = lax.axis_index("sp")
    tp = lax.axis_index("tp")
    z, x = sp // X, sp % X
    core, yy = tp % 2, tp // 2
    sib = tp + 1 - 2 * core
    ynb = (1 - yy) * 2 + core
    ysib = (1 - yy) * 2 + 1 - core
    xnb = z * X + 1 - x
    low, high = sp - X, sp + X
    has_low, has_high = z > 0, z < Z - 1
    has_prev, has_next = sp > 0, sp < S - 1

    kw = 2 * HEAD_DIM
    win[sp, :, 0:qw] = wq_ref[...]
    win[sp, :, qw:qw + kw] = jnp.concatenate([wk_ref[...], wv_ref[...]], axis=1)
    for part, ref in enumerate((wpost_ref, wpre_ref, wcin_ref)):
        win[sp, :, qw + kw + part * cw:qw + kw + (part + 1) * cw] = ref[...]

    barrier = pltpu.get_barrier_semaphore()

    def greet(dev):
        pl.semaphore_signal(barrier, inc=1, device_id=dev, device_id_type=MESH)

    greet((xnb, tp))
    greet((sp, sib))
    greet((sp, ynb))
    for cond, dev in ((has_low, low), (has_high, high), (has_prev, sp - 1), (has_next, sp + 1)):
        @pl.when(cond)
        def _(dev=dev):
            greet((dev, tp))
    peers = 3
    for cond in (has_low, has_high, has_prev, has_next):
        peers = peers + jnp.where(cond, 1, 0)
    pl.semaphore_wait(barrier, peers)

    def remote(src, dst, ssem, rsem, dev):
        return pltpu.make_async_remote_copy(
            src_ref=src, dst_ref=dst, send_sem=ssem, recv_sem=rsem,
            device_id=dev, device_id_type=MESH,
        )

    targets = (low, high, xnb)

    def in_copy(slot, half, direction):
        block = win.at[slot, pl.ds(half * piece, piece)]
        return remote(
            block, block, in_send.at[direction, half, slot], in_recv.at[half, slot], (targets[direction], tp)
        )

    def weight_copy(kind, slot, direction, own=False):
        buf, ssem, rsem, ref = ((woa, oa_send, oa_recv, oa_ref), (woc, oc_send, oc_recv, oc_ref))[kind - 1]
        source = ref if own else buf.at[slot]
        return remote(source, buf.at[slot], ssem.at[direction, slot], rsem.at[slot], (targets[direction], tp))

    weight_copy(2, sp, 2, True).start()
    for half in range(2):
        for direction, cond in ((0, has_low), (1, has_high)):
            @pl.when(cond)
            def _(half=half, direction=direction):
                in_copy(sp, half, direction).start()
        in_copy(sp, half, 2).start()

    tok_y = remote(tok_ref, tok.at[tp], tok_sem.at[0], tok_sem.at[1], (sp, ynb))
    tok_y.start()
    tok_s = remote(tok_ref, tok.at[tp], tok_sem.at[2], tok_sem.at[3], (sp, sib))
    tok_s.start()
    local = [
        pltpu.make_async_copy(tok_ref, tok.at[tp], loc_sem.at[0]),
        pltpu.make_async_copy(oa_ref, woa.at[sp], loc_sem.at[2]),
        pltpu.make_async_copy(oc_ref, woc.at[sp], loc_sem.at[3]),
    ]
    for copy in local:
        copy.start()

    MB = 128
    quarter = HEAD_DIM // 4

    def angles(i, carry):
        r = pl.ds(pl.multiple_of(i * MB, MB), MB)
        pos = sp * rows + i * MB + lax.broadcasted_iota(jnp.int32, (MB, kw), 0)
        lane = lax.broadcasted_iota(jnp.int32, (MB, kw), 1) % HEAD_DIM
        freq = jnp.exp((lane % quarter).astype(jnp.float32) * (-4.0 / HEAD_DIM * math.log(rope_base)))
        index = jnp.where(lane >= 2 * quarter, pos % GRID_W, pos // GRID_W)
        angle = index.astype(jnp.float32) * freq
        cos_ref[r, :] = jnp.cos(angle)
        sin_ref[r, :] = jnp.where(lane % (2 * quarter) < quarter, -1.0, 1.0) * jnp.sin(angle)
        return carry

    lax.fori_loop(0, rows // MB, angles, 0)
    for copy in local:
        copy.wait()
    remote(tok.at[ynb], tok.at[ynb], tok_sem.at[0], tok_sem.at[1], (sp, ynb)).wait_recv()
    tok_f = remote(tok.at[ynb], tok.at[ynb], tok_sem.at[4], tok_sem.at[5], (sp, sib))
    tok_f.start()
    remote(tok.at[sib], tok.at[sib], tok_sem.at[2], tok_sem.at[3], (sp, sib)).wait_recv()
    remote(tok.at[ysib], tok.at[ysib], tok_sem.at[4], tok_sem.at[5], (sp, sib)).wait_recv()

    TP = tok.shape[0]
    RB = 64

    def norm_rows(i, carry):
        r = pl.ds(pl.multiple_of(i * RB, RB), RB)
        total = jnp.zeros((RB, 1), jnp.float32)
        for t in range(TP):
            v = tok[t, r, :].astype(jnp.float32)
            total += jnp.sum(v * v, axis=1, keepdims=True)
        scale = lax.rsqrt(total / (TP * width) + norm_eps)
        for t in range(TP):
            v = tok[t, r, :].astype(jnp.float32)
            g = gain_ref[:, t * width:(t + 1) * width]
            normed[r, t * width:(t + 1) * width] = (v * scale * g).astype(jnp.bfloat16)
        return carry

    lax.fori_loop(0, rows // RB, norm_rows, 0)

    def project(slot, first):
        def body(i, carry):
            r = pl.ds(pl.multiple_of(i * MB, MB), MB)
            c = pl.ds(pl.multiple_of(slot * depth, depth), depth)
            prod = jnp.dot(normed[r, c], win[slot], preferred_element_type=jnp.float32)
            if first:
                acc[r, :] = prod
            else:
                acc[r, :] += prod
            return carry
        lax.fori_loop(0, rows // MB, body, 0)

    def entry(k):
        dist = (k + 1) // 2
        up = 1 - k % 2
        zz = z + dist * (2 * up - 1)
        return zz, up, (zz >= 0) & (zz < Z)

    def wait_weight(kind, slot):
        weight_copy(kind, slot, 2).wait_recv()

    def pass_on(kind, slot, up, across):
        @pl.when((up == 1) & has_low)
        def _():
            weight_copy(kind, slot, 0).start()
        @pl.when((up == 0) & has_high)
        def _():
            weight_copy(kind, slot, 1).start()
        if across:
            weight_copy(kind, slot, 2).start()

    entries = 2 * Z - 1

    def start_out_weights():
        for direction, cond in ((0, has_low), (1, has_high)):
            @pl.when(cond)
            def _(direction=direction):
                weight_copy(1, sp, direction, True).start()
                weight_copy(2, sp, direction, True).start()
        weight_copy(1, sp, 2, True).start()
        wait_weight(2, xnb)
        for direction, cond in ((0, has_low), (1, has_high)):
            @pl.when(cond)
            def _(direction=direction):
                weight_copy(2, xnb, direction).start()

    project(sp, True)

    def out_comm(dist):
        for kind, across, far in ((1, True, False), (2, False, False), (2, False, True)):
            for up in (0, 1):
                zz = z + dist * (2 * up - 1)

                @pl.when((zz >= 0) & (zz < Z))
                def _(zz=zz, up=up, kind=kind, across=across, far=far):
                    slot = zz * X + (1 - x if far else x)
                    wait_weight(kind, slot)
                    pass_on(kind, slot, up, across)

    def in_step(dist, carry):
        for half in range(2):
            for up in (0, 1):
                zz = z + dist * (2 * up - 1)

                @pl.when((zz >= 0) & (zz < Z))
                def _(zz=zz, half=half, up=up):
                    slot = zz * X + x
                    in_copy(slot, half, 2).wait_recv()
                    @pl.when(has_low if up else has_high)
                    def _():
                        in_copy(slot, half, 0 if up else 1).start()
                    in_copy(slot, half, 2).start()

        @pl.when(dist == Z - 2)
        def _():
            start_out_weights()

        @pl.when(dist == Z - 1)
        def _():
            out_comm(1)

        def work(side, carry):
            zz = z + dist * (2 * side - 1)

            @pl.when((zz >= 0) & (zz < Z))
            def _():
                project(zz * X + x, False)
            zo = z + (dist - 1) * (2 * side - 1)

            @pl.when((zo >= 0) & (zo < Z) & ((dist > 1) | (side == 0)))
            def _():
                slot = zo * X + 1 - x
                for half in range(2):
                    in_copy(slot, half, 2).wait_recv()
                project(slot, False)
            return carry

        lax.fori_loop(0, 2, work, 0)
        return carry

    lax.fori_loop(1, Z + 1, in_step, 0)

    def turned(v, cosv, sinv):
        lane = lax.broadcasted_iota(jnp.int32, v.shape, 1)
        partner = jnp.where(
            lane % (2 * quarter) < quarter,
            pltpu.roll(v, v.shape[1] - quarter, 1),
            pltpu.roll(v, quarter, 1),
        )
        return v * cosv + partner * sinv

    def kv_rows(i, carry):
        r = pl.ds(pl.multiple_of(i * MB, MB), MB)
        v = acc[r, qw:qw + kw]
        lane = lax.broadcasted_iota(jnp.int32, v.shape, 1)
        kv = jnp.where(lane < HEAD_DIM, turned(v, cos_ref[r, :], sin_ref[r, :]), v)
        kvp[pl.ds(pl.multiple_of(WINDOW + i * MB, MB), MB), :] = kv.astype(jnp.bfloat16)
        base = qw + kw + cw
        mi = (acc[r, base:base + cw] * acc[r, base + cw:base + 2 * cw]).astype(jnp.bfloat16)
        cf[pl.ds(pl.multiple_of(8 + i * MB, 8), MB), :] = mi.astype(jnp.float32)
        return carry

    lax.fori_loop(0, rows // MB, kv_rows, 0)
    E = chalo_out.shape[1]
    chalo_out[0] = cf[8:8 + E, :].astype(jnp.bfloat16)
    chalo_out[1] = cf[8 + rows - E:8 + rows, :].astype(jnp.bfloat16)

    to_next = [
        remote(kvp.at[pl.ds(rows, WINDOW)], kvp.at[pl.ds(0, WINDOW)], halo_sem.at[0], halo_sem.at[1], (sp + 1, tp)),
        remote(chalo_out.at[1], chalo_in.at[0], halo_sem.at[2], halo_sem.at[3], (sp + 1, tp)),
    ]
    to_prev = [
        remote(kvp.at[pl.ds(WINDOW, WINDOW)], kvp.at[pl.ds(WINDOW + rows, WINDOW)], halo_sem.at[4], halo_sem.at[5], (sp - 1, tp)),
        remote(chalo_out.at[0], chalo_in.at[1], halo_sem.at[6], halo_sem.at[7], (sp - 1, tp)),
    ]

    @pl.when(has_next)
    def _():
        for copy in to_next:
            copy.start()

    @pl.when(has_prev)
    def _():
        for copy in to_prev:
            copy.start()

    if Z > 2:
        out_comm(2)

    def q_rows(i, carry):
        r = pl.ds(pl.multiple_of(i * MB, MB), MB)
        for c in range(qw // kw):
            qbuf[r, c * kw:(c + 1) * kw] = turned(
                acc[r, c * kw:(c + 1) * kw], cos_ref[r, :], sin_ref[r, :]
            ).astype(jnp.bfloat16)
        return carry

    lax.fori_loop(0, rows // MB, q_rows, 0)

    zero_kv = jnp.zeros((WINDOW, kw), jnp.bfloat16)
    zero_c = jnp.zeros((8, cw), jnp.float32)

    @pl.when(has_prev)
    def _():
        for copy in to_next:
            copy.wait_recv()
        cf[0:8, :] = chalo_in[0, E - 8:E, :].astype(jnp.float32)

    @pl.when(jnp.logical_not(has_prev))
    def _():
        kvp[0:WINDOW, :] = zero_kv
        cf[0:8, :] = zero_c

    @pl.when(has_next)
    def _():
        for copy in to_prev:
            copy.wait_recv()
        cf[8 + rows:16 + rows, :] = chalo_in[1, 0:8, :].astype(jnp.float32)

    @pl.when(jnp.logical_not(has_next))
    def _():
        kvp[WINDOW + rows:, :] = zero_kv
        cf[8 + rows:16 + rows, :] = zero_c

    taps = [taps_ref[t:t + 1, :] for t in range(3)]
    for i in range(rows // MB):
        a = 8 + i * MB
        conv = (
            taps[0] * cf[a - 1:a - 1 + MB, :]
            + taps[1] * cf[a:a + MB, :]
            + taps[2] * cf[a + 1:a + 1 + MB, :]
        )
        cout[i * MB:(i + 1) * MB, :] = (acc[i * MB:(i + 1) * MB, qw + kw:qw + kw + cw] * conv).astype(jnp.bfloat16)

    heads = qw // HEAD_DIM
    K3 = 3 * WINDOW
    total_tokens = rows * S

    def attend(b, carry):
        r = pl.ds(pl.multiple_of(b * WINDOW, WINDOW), WINDOW)
        kv = kvp[pl.ds(pl.multiple_of(b * WINDOW, WINDOW), K3), :].astype(jnp.float32)
        lane = lax.broadcasted_iota(jnp.int32, (K3, kw), 1)
        swapped = pltpu.roll(kv, HEAD_DIM, 1)
        kk = jnp.where(lane < HEAD_DIM, kv, swapped).astype(jnp.bfloat16)
        vv = jnp.where(lane < HEAD_DIM, swapped, kv).astype(jnp.bfloat16)
        k_half = [jnp.where(lane < HEAD_DIM, kk, 0), jnp.where(lane < HEAD_DIM, 0, kk)]
        v_half = [jnp.where(lane < HEAD_DIM, vv, 0), jnp.where(lane < HEAD_DIM, 0, vv)]
        qi = lax.broadcasted_iota(jnp.int32, (WINDOW, K3), 0)
        ki = lax.broadcasted_iota(jnp.int32, (WINDOW, K3), 1)
        first = sp * rows + b * WINDOW - WINDOW
        allowed = (ki >= qi) & (ki <= qi + 2 * WINDOW) & (ki + first >= 0) & (ki + first < total_tokens)
        lse_lane = lax.broadcasted_iota(jnp.int32, (WINDOW, WINDOW), 1)
        lse_all = jnp.zeros((WINDOW, WINDOW), jnp.float32)
        for pair in range(heads // 2):
            q = qbuf[r, pair * kw:(pair + 1) * kw]
            total = jnp.zeros((WINDOW, kw), jnp.float32)
            for side in range(2):
                h = pair * 2 + side
                s = lax.dot_general(
                    q, k_half[side], (((1,), (1,)), ((), ())), preferred_element_type=jnp.float32
                ) * HEAD_DIM ** (-0.5)
                s = jnp.where(allowed, s, -jnp.inf)
                sink = sink_ref[h]
                top = jnp.maximum(jnp.max(s, axis=1, keepdims=True), sink)
                e = jnp.exp(s - top)
                den = jnp.sum(e, axis=1, keepdims=True) + jnp.exp(sink - top)
                w = (e * (1.0 / den)).astype(jnp.bfloat16)
                total += jnp.dot(w, v_half[side], preferred_element_type=jnp.float32)
                lse_all = jnp.where(lse_lane == h, top + jnp.log(den), lse_all)
            att[r, pair * kw:(pair + 1) * kw] = total.astype(jnp.bfloat16)
        lse_ref[:, r] = jnp.transpose(lse_all)[0:heads, :]
        return carry

    blocks = rows // WINDOW
    lax.fori_loop(0, blocks, attend, 0)

    chunk = rows // TP

    def sib_copy(slot):
        return remote(part_send.at[slot], part_recv.at[slot], rs_sem.at[0, slot], rs_sem.at[1, slot], (sp, sib))

    def y_copy(slot):
        return remote(y_send.at[slot], y_recv.at[slot], rs_sem.at[2, slot], rs_sem.at[3, slot], (sp, ynb))

    def out_block(slot):
        for half in range(2):
            for mine in range(2):
                t = half * 2 + (core if mine else 1 - core)
                r = pl.ds(pl.multiple_of(t * chunk, chunk), chunk)
                v = jnp.dot(att[r, :], woa[slot], preferred_element_type=jnp.float32) + jnp.dot(
                    cout[r, :], woc[slot], preferred_element_type=jnp.float32
                )
                if mine:
                    part_keep[slot, half] = v
                else:
                    part_send[slot, half] = v.astype(jnp.bfloat16)
        sib_copy(slot).start()

    def y_block(slot):
        sib_copy(slot).wait_recv()
        y_send[slot] = (
            part_keep[slot, 1 - yy] + part_recv[slot, 1 - yy].astype(jnp.float32)
        ).astype(jnp.bfloat16)
        y_copy(slot).start()

    def finish(slot):
        y_copy(slot).wait_recv()
        out_ref[:, pl.ds(pl.multiple_of(slot * cols, cols), cols)] = (
            part_keep[slot, yy]
            + part_recv[slot, yy].astype(jnp.float32)
            + y_recv[slot].astype(jnp.float32)
        ).astype(jnp.bfloat16)

    def each(fn, lo, hi):
        def step(u, carry):
            k, side = u // 2, u % 2
            zz, _, valid = entry(k)

            @pl.when(valid)
            def _():
                slot = zz * X + jnp.where(side == 0, x, 1 - x)
                fn(slot, k, side)
            return carry
        lax.fori_loop(lo, hi, step, 0)

    def project_out(slot, k, side):
        @pl.when(side == 1)
        def _():
            wait_weight(1, slot)
        out_block(slot)

    early = min(6, 2 * entries)
    each(project_out, 0, early)
    each(lambda slot, k, side: y_block(slot), 0, early)
    for dist in range(3, Z):
        out_comm(dist)
    each(project_out, early, 2 * entries)
    each(lambda slot, k, side: y_block(slot), early, 2 * entries)
    each(lambda slot, k, side: finish(slot), 0, 2 * entries)

    tok_y.wait_send()
    tok_s.wait_send()
    tok_f.wait_send()

    @pl.when(has_next)
    def _():
        for copy in to_next:
            copy.wait_send()

    @pl.when(has_prev)
    def _():
        for copy in to_prev:
            copy.wait_send()

    def drain(zz, carry):
        mine, other = zz * X + x, zz * X + 1 - x
        for direction, cond in ((0, (zz >= z) & has_low), (1, (zz <= z) & has_high)):
            @pl.when(cond)
            def _(direction=direction):
                in_copy(mine, 0, direction).wait_send()
                in_copy(mine, 1, direction).wait_send()
                weight_copy(1, mine, direction).wait_send()
                weight_copy(2, mine, direction).wait_send()
                weight_copy(2, other, direction).wait_send()
        in_copy(mine, 0, 2).wait_send()
        in_copy(mine, 1, 2).wait_send()
        weight_copy(1, mine, 2).wait_send()
        for slot in (mine, other):
            sib_copy(slot).wait_send()
            y_copy(slot).wait_send()
        return carry

    lax.fori_loop(0, Z, drain, 0)
    weight_copy(2, sp, 2).wait_send()


def fused(
    tokens, norm_gain, w_query, w_key, w_value, w_post_gate, w_pre_gate, w_conv_in,
    conv_taps, sink_logit, w_out_attn, w_out_conv,
):
    S, TP = lax.axis_size("sp"), lax.axis_size("tp")
    X = 2
    Z = S // X
    rows, width = tokens.shape
    depth, qw = w_query.shape
    cw = w_post_gate.shape[1]
    cols = w_out_attn.shape[1]
    heads = qw // HEAD_DIM
    kw = 2 * HEAD_DIM
    nw = qw + kw + 3 * cw
    chunk = rows // TP
    bf, f32 = jnp.bfloat16, jnp.float32
    dma = pltpu.SemaphoreType.DMA
    return pl.pallas_call(
        functools.partial(fused_kernel, Z, X),
        out_shape=(
            jax.ShapeDtypeStruct((chunk, S * cols), bf),
            jax.ShapeDtypeStruct((heads, rows), f32),
        ),
        in_specs=[pl.BlockSpec(memory_space=pltpu.VMEM)] * 11 + [pl.BlockSpec(memory_space=pltpu.SMEM)],
        out_specs=(pl.BlockSpec(memory_space=pltpu.VMEM),) * 2,
        scratch_shapes=[
            pltpu.VMEM((rows, kw), f32),
            pltpu.VMEM((rows, kw), f32),
            pltpu.VMEM((TP, rows, width), bf),
            pltpu.VMEM((rows, TP * width), bf),
            pltpu.VMEM((S, depth, nw), bf),
            pltpu.VMEM((S,) + w_out_attn.shape, bf),
            pltpu.VMEM((S,) + w_out_conv.shape, bf),
            pltpu.VMEM((rows, nw), f32),
            pltpu.VMEM((rows, qw), bf),
            pltpu.VMEM((rows + 2 * WINDOW, kw), bf),
            pltpu.VMEM((rows + 16, cw), f32),
            pltpu.VMEM((2, 16, cw), bf),
            pltpu.VMEM((2, 16, cw), bf),
            pltpu.VMEM((rows, qw), bf),
            pltpu.VMEM((rows, cw), bf),
            pltpu.VMEM((S, 2, chunk, cols), f32),
            pltpu.VMEM((S, 2, chunk, cols), bf),
            pltpu.VMEM((S, 2, chunk, cols), bf),
            pltpu.VMEM((S, chunk, cols), bf),
            pltpu.VMEM((S, chunk, cols), bf),
            dma((6,)),
            dma((3, 2, S)), dma((2, S)),
            dma((3, S)), dma((S,)),
            dma((3, S)), dma((S,)),
            dma((8,)),
            dma((4, S)),
            dma((4,)),
        ],
        compiler_params=pltpu.CompilerParams(
            collective_id=0, has_side_effects=True, vmem_limit_bytes=60 * 1024 * 1024
        ),
    )(
        tokens, norm_gain[None, :], w_query, w_key, w_value, w_post_gate, w_pre_gate, w_conv_in,
        w_out_attn, w_out_conv, conv_taps, sink_logit,
    )


def fits(
    tokens, norm_gain, w_query, w_key, w_value, w_post_gate, w_pre_gate, w_conv_in,
    conv_taps, sink_logit, w_out_attn, w_out_conv,
):
    S, TP = lax.axis_size("sp"), lax.axis_size("tp")
    return (
        TP == 4
        and S % 2 == 0
        and S >= 6
        and w_key.shape[1] == HEAD_DIM
        and w_query.shape[0] % 128 == 0
        and w_query.shape[1] % 128 == 0
        and w_post_gate.shape[1] % 128 == 0
        and w_out_attn.shape[1] % 128 == 0
        and tokens.shape[0] % (TP * WINDOW) == 0
        and tokens.shape[1] % 128 == 0
    )


def either(*args):
    return fused(*args) if fits(*args) else on_device(*args)


def solution(mesh):
    placed = (
        P("sp", "tp"),
        P(),
        P("sp", "tp"),
        P("sp", "tp"),
        P("sp", "tp"),
        P("sp", "tp"),
        P("sp", "tp"),
        P("sp", "tp"),
        P(None, "tp"),
        P("tp"),
        P("tp", "sp"),
        P("tp", "sp"),
    )
    return jax.shard_map(
        either,
        mesh=mesh,
        in_specs=placed,
        out_specs=(P(("sp", "tp"), None), P("tp", "sp")),
        check_vma=False,
    )
```

```python
import functools
import math

import jax
import jax.numpy as jnp
from jax import lax
from jax.experimental import pallas as pl
from jax.experimental.pallas import tpu as pltpu
from jax.sharding import PartitionSpec as P

MESH = pl.DeviceIdType.MESH

HEAD_DIM = 64
WINDOW = 128
GRID_W = 64


rope_base = 10000.0
norm_eps = 1e-06


def padded(block, sides, width):
    for axis, dim in sides:
        count = lax.axis_size(axis)
        forward = [(i, i + 1) for i in range(count - 1)]
        backward = [(target, source) for source, target in forward]
        low = lax.ppermute(
            lax.slice_in_dim(block, block.shape[dim] - width, None, axis=dim), axis, forward
        )
        high = lax.ppermute(lax.slice_in_dim(block, 0, width, axis=dim), axis, backward)
        block = jnp.concatenate([low, block, high], axis=dim)
    return block


def rotate_pair(values, angles):
    first_half, second_half = jnp.split(values, 2, axis=-1)
    cosine = jnp.cos(angles)[:, None, :]
    sine_part = jnp.sin(angles)[:, None, :]
    return jnp.concatenate(
        [
            first_half * cosine - second_half * sine_part,
            first_half * sine_part + second_half * cosine,
        ],
        axis=-1,
    )


def axial_rotate(values, positions):
    half_dim = values.shape[-1] // 2
    inv_freq = rope_base ** (-jnp.arange(0, half_dim, 2).astype(jnp.float32) / half_dim)
    row_angle = (positions // GRID_W).astype(jnp.float32)[:, None] * inv_freq
    col_angle = (positions % GRID_W).astype(jnp.float32)[:, None] * inv_freq
    row_part, col_part = jnp.split(values, 2, axis=-1)
    return jnp.concatenate(
        [rotate_pair(row_part, row_angle), rotate_pair(col_part, col_angle)], axis=-1
    )


def block_windows(source, rows_local, blocks):
    pieces = [
        source[step * WINDOW : step * WINDOW + rows_local].reshape(
            (blocks, WINDOW) + source.shape[1:]
        )
        for step in range(3)
    ]
    return jnp.concatenate(pieces, axis=1)


def on_device(
    tokens,
    norm_gain,
    w_query,
    w_key,
    w_value,
    w_post_gate,
    w_pre_gate,
    w_conv_in,
    conv_taps,
    sink_logit,
    w_out_attn,
    w_out_conv,
):
    whole = lax.all_gather(tokens, "tp", axis=1, tiled=True)
    rows_local = whole.shape[0]
    whole_float = whole.astype(jnp.float32)
    mean_square = jnp.mean(whole_float * whole_float, axis=1, keepdims=True)
    normed = (whole_float * lax.rsqrt(mean_square + norm_eps) * norm_gain).astype(jnp.bfloat16)
    col_widths = [
        w_query.shape[1],
        w_key.shape[1],
        w_value.shape[1],
        w_post_gate.shape[1],
        w_pre_gate.shape[1],
        w_conv_in.shape[1],
    ]
    joined = jnp.concatenate(
        (
            lax.all_gather(w_query, "sp", axis=0, tiled=True),
            lax.all_gather(w_key, "sp", axis=0, tiled=True),
            lax.all_gather(w_value, "sp", axis=0, tiled=True),
            lax.all_gather(w_post_gate, "sp", axis=0, tiled=True),
            lax.all_gather(w_pre_gate, "sp", axis=0, tiled=True),
            lax.all_gather(w_conv_in, "sp", axis=0, tiled=True),
        ),
        axis=1,
    )
    projected = jnp.dot(normed, joined, preferred_element_type=jnp.float32)
    bounds = []
    running = 0
    for col_width in col_widths[:-1]:
        running += col_width
        bounds.append(running)
    query_raw, key_raw, value_raw, post_gate, pre_gate, conv_input = jnp.split(
        projected, bounds, axis=1
    )
    offset = lax.axis_index("sp") * rows_local
    positions = offset + jnp.arange(rows_local, dtype=jnp.int32)
    local_heads = w_query.shape[1] // HEAD_DIM
    local_groups = w_key.shape[1] // HEAD_DIM
    group_size = local_heads // local_groups
    queries = axial_rotate(query_raw.reshape(rows_local, local_heads, HEAD_DIM), positions).astype(
        jnp.bfloat16
    )
    keys_rot = axial_rotate(key_raw.reshape(rows_local, local_groups, HEAD_DIM), positions).astype(
        jnp.bfloat16
    )
    key_value = jnp.concatenate(
        [keys_rot.reshape(rows_local, local_groups * HEAD_DIM), value_raw.astype(jnp.bfloat16)],
        axis=1,
    )
    mixed_input = (pre_gate * conv_input).astype(jnp.bfloat16)
    kv_padded = padded(key_value, (("sp", 0),), WINDOW)
    conv_padded = padded(mixed_input, (("sp", 0),), 1)
    conv_float = conv_padded.astype(jnp.float32)
    convolved = (
        conv_taps[0] * conv_float[:-2]
        + conv_taps[1] * conv_float[1:-1]
        + conv_taps[2] * conv_float[2:]
    )
    conv_out = (post_gate * convolved).astype(jnp.bfloat16)
    total_tokens = rows_local * lax.axis_size("sp")
    blocks = rows_local // WINDOW
    padded_rows = rows_local + 2 * WINDOW
    block_queries = queries.reshape(blocks, WINDOW, local_groups, group_size, HEAD_DIM)
    block_keys = block_windows(
        kv_padded[:, : local_groups * HEAD_DIM].reshape(padded_rows, local_groups, HEAD_DIM),
        rows_local,
        blocks,
    )
    block_values = block_windows(
        kv_padded[:, local_groups * HEAD_DIM :].reshape(padded_rows, local_groups, HEAD_DIM),
        rows_local,
        blocks,
    )
    scores = jnp.einsum(
        "nqkgd,nskd->nkgqs", block_queries, block_keys, preferred_element_type=jnp.float32
    ) * HEAD_DIM ** (-0.5)
    query_pos = positions.reshape(blocks, WINDOW)
    key_pos = (
        offset
        - WINDOW
        + (jnp.arange(blocks, dtype=jnp.int32) * WINDOW)[:, None]
        + jnp.arange(3 * WINDOW, dtype=jnp.int32)[None, :]
    )
    distance = key_pos[:, None, :] - query_pos[:, :, None]
    allowed = (
        (jnp.abs(distance) <= WINDOW)
        & (key_pos >= 0)[:, None, :]
        & (key_pos < total_tokens)[:, None, :]
    )
    scores = jnp.where(allowed[:, None, None], scores, -jnp.inf)
    sink_values = sink_logit.reshape(local_groups, group_size)[None, :, :, None]
    row_max = jnp.maximum(jnp.max(scores, axis=-1), sink_values)
    exp_scores = jnp.exp(scores - row_max[..., None])
    denominator = jnp.sum(exp_scores, axis=-1) + jnp.exp(sink_values - row_max)
    weights = (exp_scores / denominator[..., None]).astype(jnp.bfloat16)
    attended = (
        jnp.einsum("nkgqs,nskd->nqkgd", weights, block_values, preferred_element_type=jnp.float32)
        .astype(jnp.bfloat16)
        .reshape(rows_local, local_heads * HEAD_DIM)
    )
    log_sum = row_max + jnp.log(denominator)
    log_weight_sum = jnp.transpose(log_sum, (1, 2, 0, 3)).reshape(local_heads, rows_local)
    out_attn, out_conv = (
        lax.all_gather(w_out_attn, "sp", axis=1, tiled=True),
        lax.all_gather(w_out_conv, "sp", axis=1, tiled=True),
    )
    mixed = lax.psum_scatter(
        (
            jnp.dot(attended, out_attn, preferred_element_type=jnp.float32)
            + jnp.dot(conv_out, out_conv, preferred_element_type=jnp.float32)
        ).astype(jnp.bfloat16),
        "tp",
        scatter_dimension=0,
        tiled=True,
    )
    return (mixed, log_weight_sum)


def fused_kernel(
    Z, X,
    tok_ref, gain_ref, wq_ref, wk_ref, wv_ref, wpost_ref, wpre_ref, wcin_ref, oa_ref, oc_ref, taps_ref, sink_ref,
    out_ref, lse_ref,
    cos_ref, sin_ref, tok, normed, win, woa, woc, acc, qbuf, kvp, cf, chalo_out, chalo_in, att, cout,
    part_keep, part_send, part_recv, y_send, y_recv,
    tok_sem, in_send, in_recv, oa_send, oa_recv, oc_send, oc_recv, halo_sem, rs_sem, loc_sem,
):
    S = Z * X
    rows, width = tok_ref.shape
    depth = wq_ref.shape[0]
    piece = depth // 2
    cols = oa_ref.shape[1]
    qw = qbuf.shape[1]
    cw = cf.shape[1]
    sp = lax.axis_index("sp")
    tp = lax.axis_index("tp")
    z, x = sp // X, sp % X
    core, yy = tp % 2, tp // 2
    sib = tp + 1 - 2 * core
    ynb = (1 - yy) * 2 + core
    ysib = (1 - yy) * 2 + 1 - core
    xnb = z * X + 1 - x
    low, high = sp - X, sp + X
    has_low, has_high = z > 0, z < Z - 1
    has_prev, has_next = sp > 0, sp < S - 1

    kw = 2 * HEAD_DIM
    win[sp, :, 0:qw] = wq_ref[...]
    kv_t = jnp.concatenate([wk_ref[...], wv_ref[...]], axis=0).astype(jnp.float32)
    win[sp, :, qw:qw + kw] = jnp.transpose(kv_t).astype(jnp.bfloat16)
    for part, ref in enumerate((wpost_ref, wpre_ref, wcin_ref)):
        win[sp, :, qw + kw + part * cw:qw + kw + (part + 1) * cw] = ref[...]

    barrier = pltpu.get_barrier_semaphore()

    def greet(dev):
        pl.semaphore_signal(barrier, inc=1, device_id=dev, device_id_type=MESH)

    greet((xnb, tp))
    greet((sp, sib))
    greet((sp, ynb))
    for cond, dev in ((has_low, low), (has_high, high), (has_prev, sp - 1), (has_next, sp + 1)):
        @pl.when(cond)
        def _(dev=dev):
            greet((dev, tp))
    peers = 3
    for cond in (has_low, has_high, has_prev, has_next):
        peers = peers + jnp.where(cond, 1, 0)
    pl.semaphore_wait(barrier, peers)

    def remote(src, dst, ssem, rsem, dev):
        return pltpu.make_async_remote_copy(
            src_ref=src, dst_ref=dst, send_sem=ssem, recv_sem=rsem,
            device_id=dev, device_id_type=MESH,
        )

    targets = (low, high, xnb)

    def in_copy(slot, half, direction):
        block = win.at[slot, pl.ds(half * piece, piece)]
        return remote(
            block, block, in_send.at[direction, half, slot], in_recv.at[half, slot], (targets[direction], tp)
        )

    def weight_copy(kind, slot, direction, own=False):
        buf, ssem, rsem, ref = ((woa, oa_send, oa_recv, oa_ref), (woc, oc_send, oc_recv, oc_ref))[kind - 1]
        source = ref if own else buf.at[slot]
        return remote(source, buf.at[slot], ssem.at[direction, slot], rsem.at[slot], (targets[direction], tp))

    weight_copy(2, sp, 2, True).start()
    for half in range(2):
        for direction, cond in ((0, has_low), (1, has_high)):
            @pl.when(cond)
            def _(half=half, direction=direction):
                in_copy(sp, half, direction).start()
        in_copy(sp, half, 2).start()

    tok_y = remote(tok_ref, tok.at[tp], tok_sem.at[0], tok_sem.at[1], (sp, ynb))
    tok_y.start()
    tok_s = remote(tok_ref, tok.at[tp], tok_sem.at[2], tok_sem.at[3], (sp, sib))
    tok_s.start()
    local = [
        pltpu.make_async_copy(tok_ref, tok.at[tp], loc_sem.at[0]),
        pltpu.make_async_copy(oa_ref, woa.at[sp], loc_sem.at[2]),
        pltpu.make_async_copy(oc_ref, woc.at[sp], loc_sem.at[3]),
    ]
    for copy in local:
        copy.start()

    MB = 128
    quarter = HEAD_DIM // 4

    def angles(i, carry):
        r = pl.ds(pl.multiple_of(i * MB, MB), MB)
        pos = sp * rows + i * MB + lax.broadcasted_iota(jnp.int32, (MB, kw), 0)
        lane = lax.broadcasted_iota(jnp.int32, (MB, kw), 1) % HEAD_DIM
        freq = jnp.exp((lane % quarter).astype(jnp.float32) * (-4.0 / HEAD_DIM * math.log(rope_base)))
        index = jnp.where(lane >= 2 * quarter, pos % GRID_W, pos // GRID_W)
        angle = index.astype(jnp.float32) * freq
        cos_ref[r, :] = jnp.cos(angle)
        sin_ref[r, :] = jnp.where(lane % (2 * quarter) < quarter, -1.0, 1.0) * jnp.sin(angle)
        return carry

    lax.fori_loop(0, rows // MB, angles, 0)

    def in_comm(dist):
        for half in range(2):
            for up in (0, 1):
                zz = z + dist * (2 * up - 1)

                @pl.when((zz >= 0) & (zz < Z))
                def _(zz=zz, half=half, up=up):
                    slot = zz * X + x
                    in_copy(slot, half, 2).wait_recv()
                    @pl.when(has_low if up else has_high)
                    def _():
                        in_copy(slot, half, 0 if up else 1).start()
                    in_copy(slot, half, 2).start()

    in_comm(1)
    for copy in local:
        copy.wait()
    remote(tok.at[ynb], tok.at[ynb], tok_sem.at[0], tok_sem.at[1], (sp, ynb)).wait_recv()
    tok_f = remote(tok.at[ynb], tok.at[ynb], tok_sem.at[4], tok_sem.at[5], (sp, sib))
    tok_f.start()
    remote(tok.at[sib], tok.at[sib], tok_sem.at[2], tok_sem.at[3], (sp, sib)).wait_recv()
    remote(tok.at[ysib], tok.at[ysib], tok_sem.at[4], tok_sem.at[5], (sp, sib)).wait_recv()

    TP = tok.shape[0]
    RB = 64

    def norm_rows(i, carry):
        r = pl.ds(pl.multiple_of(i * RB, RB), RB)
        total = jnp.zeros((RB, 1), jnp.float32)
        for t in range(TP):
            v = tok[t, r, :].astype(jnp.float32)
            total += jnp.sum(v * v, axis=1, keepdims=True)
        scale = lax.rsqrt(total / (TP * width) + norm_eps)
        for t in range(TP):
            v = tok[t, r, :].astype(jnp.float32)
            g = gain_ref[:, t * width:(t + 1) * width]
            normed[r, t * width:(t + 1) * width] = (v * scale * g).astype(jnp.bfloat16)
        return carry

    lax.fori_loop(0, rows // RB, norm_rows, 0)

    def project(slot, first):
        def body(i, carry):
            r = pl.ds(pl.multiple_of(i * MB, MB), MB)
            c = pl.ds(pl.multiple_of(slot * depth, depth), depth)
            prod = jnp.dot(normed[r, c], win[slot], preferred_element_type=jnp.float32)
            if first:
                acc[r, :] = prod
            else:
                acc[r, :] += prod
            return carry
        lax.fori_loop(0, rows // MB, body, 0)

    def entry(k):
        dist = (k + 1) // 2
        up = 1 - k % 2
        zz = z + dist * (2 * up - 1)
        return zz, up, (zz >= 0) & (zz < Z)

    def wait_weight(kind, slot):
        weight_copy(kind, slot, 2).wait_recv()

    def pass_on(kind, slot, up, across):
        @pl.when((up == 1) & has_low)
        def _():
            weight_copy(kind, slot, 0).start()
        @pl.when((up == 0) & has_high)
        def _():
            weight_copy(kind, slot, 1).start()
        if across:
            weight_copy(kind, slot, 2).start()

    entries = 2 * Z - 1

    def start_out_weights():
        for direction, cond in ((0, has_low), (1, has_high)):
            @pl.when(cond)
            def _(direction=direction):
                weight_copy(1, sp, direction, True).start()
                weight_copy(2, sp, direction, True).start()
        weight_copy(1, sp, 2, True).start()
        wait_weight(2, xnb)
        for direction, cond in ((0, has_low), (1, has_high)):
            @pl.when(cond)
            def _(direction=direction):
                weight_copy(2, xnb, direction).start()

    project(sp, True)

    def out_comm(dist):
        for kind, across, far in ((1, True, False), (2, False, False), (2, False, True)):
            for up in (0, 1):
                zz = z + dist * (2 * up - 1)

                @pl.when((zz >= 0) & (zz < Z))
                def _(zz=zz, up=up, kind=kind, across=across, far=far):
                    slot = zz * X + (1 - x if far else x)
                    wait_weight(kind, slot)
                    pass_on(kind, slot, up, across)

    def in_step(dist, carry):
        @pl.when(dist > 1)
        def _():
            in_comm(dist)

        @pl.when(dist == Z - 2)
        def _():
            start_out_weights()

        @pl.when(dist == Z - 1)
        def _():
            out_comm(1)

        def work(side, carry):
            zz = z + dist * (2 * side - 1)

            @pl.when((zz >= 0) & (zz < Z))
            def _():
                project(zz * X + x, False)
            zo = z + (dist - 1) * (2 * side - 1)

            @pl.when((zo >= 0) & (zo < Z) & ((dist > 1) | (side == 0)))
            def _():
                slot = zo * X + 1 - x
                for half in range(2):
                    in_copy(slot, half, 2).wait_recv()
                project(slot, False)
            return carry

        lax.fori_loop(0, 2, work, 0)
        return carry

    lax.fori_loop(1, Z + 1, in_step, 0)

    def turned(v, cosv, sinv):
        lane = lax.broadcasted_iota(jnp.int32, v.shape, 1)
        partner = jnp.where(
            lane % (2 * quarter) < quarter,
            pltpu.roll(v, v.shape[1] - quarter, 1),
            pltpu.roll(v, quarter, 1),
        )
        return v * cosv + partner * sinv

    def kv_rows(i, carry):
        r = pl.ds(pl.multiple_of(i * MB, MB), MB)
        v = acc[r, qw:qw + kw]
        lane = lax.broadcasted_iota(jnp.int32, v.shape, 1)
        kv = jnp.where(lane < HEAD_DIM, turned(v, cos_ref[r, :], sin_ref[r, :]), v)
        kvp[pl.ds(pl.multiple_of(WINDOW + i * MB, MB), MB), :] = kv.astype(jnp.bfloat16)
        base = qw + kw + cw
        mi = (acc[r, base:base + cw] * acc[r, base + cw:base + 2 * cw]).astype(jnp.bfloat16)
        cf[pl.ds(pl.multiple_of(8 + i * MB, 8), MB), :] = mi.astype(jnp.float32)
        return carry

    lax.fori_loop(0, rows // MB, kv_rows, 0)
    E = chalo_out.shape[1]
    chalo_out[0] = cf[8:8 + E, :].astype(jnp.bfloat16)
    chalo_out[1] = cf[8 + rows - E:8 + rows, :].astype(jnp.bfloat16)

    to_next = [
        remote(kvp.at[pl.ds(rows, WINDOW)], kvp.at[pl.ds(0, WINDOW)], halo_sem.at[0], halo_sem.at[1], (sp + 1, tp)),
        remote(chalo_out.at[1], chalo_in.at[0], halo_sem.at[2], halo_sem.at[3], (sp + 1, tp)),
    ]
    to_prev = [
        remote(kvp.at[pl.ds(WINDOW, WINDOW)], kvp.at[pl.ds(WINDOW + rows, WINDOW)], halo_sem.at[4], halo_sem.at[5], (sp - 1, tp)),
        remote(chalo_out.at[0], chalo_in.at[1], halo_sem.at[6], halo_sem.at[7], (sp - 1, tp)),
    ]

    @pl.when(has_next)
    def _():
        for copy in to_next:
            copy.start()

    @pl.when(has_prev)
    def _():
        for copy in to_prev:
            copy.start()

    if Z > 2:
        out_comm(2)

    def q_rows(i, carry):
        r = pl.ds(pl.multiple_of(i * MB, MB), MB)
        for c in range(qw // kw):
            qbuf[r, c * kw:(c + 1) * kw] = turned(
                acc[r, c * kw:(c + 1) * kw], cos_ref[r, :], sin_ref[r, :]
            ).astype(jnp.bfloat16)
        return carry

    lax.fori_loop(0, rows // MB, q_rows, 0)

    zero_kv = jnp.zeros((WINDOW, kw), jnp.bfloat16)
    zero_c = jnp.zeros((8, cw), jnp.float32)

    @pl.when(has_prev)
    def _():
        for copy in to_next:
            copy.wait_recv()
        cf[0:8, :] = chalo_in[0, E - 8:E, :].astype(jnp.float32)

    @pl.when(jnp.logical_not(has_prev))
    def _():
        kvp[0:WINDOW, :] = zero_kv
        cf[0:8, :] = zero_c

    @pl.when(has_next)
    def _():
        for copy in to_prev:
            copy.wait_recv()
        cf[8 + rows:16 + rows, :] = chalo_in[1, 0:8, :].astype(jnp.float32)

    @pl.when(jnp.logical_not(has_next))
    def _():
        kvp[WINDOW + rows:, :] = zero_kv
        cf[8 + rows:16 + rows, :] = zero_c

    taps = [taps_ref[t:t + 1, :] for t in range(3)]
    for i in range(rows // MB):
        a = 8 + i * MB
        conv = (
            taps[0] * cf[a - 1:a - 1 + MB, :]
            + taps[1] * cf[a:a + MB, :]
            + taps[2] * cf[a + 1:a + 1 + MB, :]
        )
        cout[i * MB:(i + 1) * MB, :] = (acc[i * MB:(i + 1) * MB, qw + kw:qw + kw + cw] * conv).astype(jnp.bfloat16)

    heads = qw // HEAD_DIM
    K3 = 3 * WINDOW
    total_tokens = rows * S

    def attend(b, carry):
        r = pl.ds(pl.multiple_of(b * WINDOW, WINDOW), WINDOW)
        kv = kvp[pl.ds(pl.multiple_of(b * WINDOW, WINDOW), K3), :].astype(jnp.float32)
        lane = lax.broadcasted_iota(jnp.int32, (K3, kw), 1)
        swapped = pltpu.roll(kv, HEAD_DIM, 1)
        kk = jnp.where(lane < HEAD_DIM, kv, swapped).astype(jnp.bfloat16)
        vv = jnp.where(lane < HEAD_DIM, swapped, kv).astype(jnp.bfloat16)
        k_half = [jnp.where(lane < HEAD_DIM, kk, 0), jnp.where(lane < HEAD_DIM, 0, kk)]
        v_half = [jnp.where(lane < HEAD_DIM, vv, 0), jnp.where(lane < HEAD_DIM, 0, vv)]
        qi = lax.broadcasted_iota(jnp.int32, (WINDOW, K3), 0)
        ki = lax.broadcasted_iota(jnp.int32, (WINDOW, K3), 1)
        first = sp * rows + b * WINDOW - WINDOW
        allowed = (ki >= qi) & (ki <= qi + 2 * WINDOW) & (ki + first >= 0) & (ki + first < total_tokens)
        lse_lane = lax.broadcasted_iota(jnp.int32, (WINDOW, WINDOW), 1)
        lse_all = jnp.zeros((WINDOW, WINDOW), jnp.float32)
        for pair in range(heads // 2):
            q = qbuf[r, pair * kw:(pair + 1) * kw]
            total = jnp.zeros((WINDOW, kw), jnp.float32)
            for side in range(2):
                h = pair * 2 + side
                s = lax.dot_general(
                    q, k_half[side], (((1,), (1,)), ((), ())), preferred_element_type=jnp.float32
                ) * HEAD_DIM ** (-0.5)
                s = jnp.where(allowed, s, -jnp.inf)
                sink = sink_ref[h]
                top = jnp.maximum(jnp.max(s, axis=1, keepdims=True), sink)
                e = jnp.exp(s - top)
                den = jnp.sum(e, axis=1, keepdims=True) + jnp.exp(sink - top)
                w = (e * (1.0 / den)).astype(jnp.bfloat16)
                total += jnp.dot(w, v_half[side], preferred_element_type=jnp.float32)
                lse_all = jnp.where(lse_lane == h, top + jnp.log(den), lse_all)
            att[r, pair * kw:(pair + 1) * kw] = total.astype(jnp.bfloat16)
        lse_ref[:, r] = jnp.transpose(lse_all)[0:heads, :]
        return carry

    blocks = rows // WINDOW
    lax.fori_loop(0, blocks, attend, 0)

    chunk = rows // TP

    def sib_copy(slot):
        return remote(part_send.at[slot], part_recv.at[slot], rs_sem.at[0, slot], rs_sem.at[1, slot], (sp, sib))

    def y_copy(slot):
        return remote(y_send.at[slot], y_recv.at[slot], rs_sem.at[2, slot], rs_sem.at[3, slot], (sp, ynb))

    def out_block(slot):
        for half in range(2):
            for mine in range(2):
                t = half * 2 + (core if mine else 1 - core)
                r = pl.ds(pl.multiple_of(t * chunk, chunk), chunk)
                v = jnp.dot(att[r, :], woa[slot], preferred_element_type=jnp.float32) + jnp.dot(
                    cout[r, :], woc[slot], preferred_element_type=jnp.float32
                )
                if mine:
                    part_keep[slot, half] = v
                else:
                    part_send[slot, half] = v.astype(jnp.bfloat16)
        sib_copy(slot).start()

    def y_block(slot):
        sib_copy(slot).wait_recv()
        y_send[slot] = (
            part_keep[slot, 1 - yy] + part_recv[slot, 1 - yy].astype(jnp.float32)
        ).astype(jnp.bfloat16)
        y_copy(slot).start()

    def finish(slot):
        y_copy(slot).wait_recv()
        out_ref[:, pl.ds(pl.multiple_of(slot * cols, cols), cols)] = (
            part_keep[slot, yy]
            + part_recv[slot, yy].astype(jnp.float32)
            + y_recv[slot].astype(jnp.float32)
        ).astype(jnp.bfloat16)

    def each(fn, lo, hi):
        def step(u, carry):
            k, side = u // 2, u % 2
            zz, _, valid = entry(k)

            @pl.when(valid)
            def _():
                slot = zz * X + jnp.where(side == 0, x, 1 - x)
                fn(slot, k, side)
            return carry
        lax.fori_loop(lo, hi, step, 0)

    def project_out(slot, k, side):
        @pl.when(side == 1)
        def _():
            wait_weight(1, slot)
        out_block(slot)

    early = min(6, 2 * entries)
    each(project_out, 0, early)
    each(lambda slot, k, side: y_block(slot), 0, early)
    for dist in range(2, Z):
        if dist > 2:
            out_comm(dist)
        lo, hi = 4 * dist - 2, 4 * dist + 2
        each(project_out, lo, hi)
        each(lambda slot, k, side: y_block(slot), lo, hi)
    each(lambda slot, k, side: finish(slot), 0, 2 * entries)

    tok_y.wait_send()
    tok_s.wait_send()
    tok_f.wait_send()

    @pl.when(has_next)
    def _():
        for copy in to_next:
            copy.wait_send()

    @pl.when(has_prev)
    def _():
        for copy in to_prev:
            copy.wait_send()

    def drain(zz, carry):
        mine, other = zz * X + x, zz * X + 1 - x
        for direction, cond in ((0, (zz >= z) & has_low), (1, (zz <= z) & has_high)):
            @pl.when(cond)
            def _(direction=direction):
                in_copy(mine, 0, direction).wait_send()
                in_copy(mine, 1, direction).wait_send()
                weight_copy(1, mine, direction).wait_send()
                weight_copy(2, mine, direction).wait_send()
                weight_copy(2, other, direction).wait_send()
        in_copy(mine, 0, 2).wait_send()
        in_copy(mine, 1, 2).wait_send()
        weight_copy(1, mine, 2).wait_send()
        for slot in (mine, other):
            sib_copy(slot).wait_send()
            y_copy(slot).wait_send()
        return carry

    lax.fori_loop(0, Z, drain, 0)
    weight_copy(2, sp, 2).wait_send()


def fused(
    tokens, norm_gain, w_query, w_key, w_value, w_post_gate, w_pre_gate, w_conv_in,
    conv_taps, sink_logit, w_out_attn, w_out_conv,
):
    S, TP = lax.axis_size("sp"), lax.axis_size("tp")
    X = 2
    Z = S // X
    rows, width = tokens.shape
    depth, qw = w_query.shape
    cw = w_post_gate.shape[1]
    cols = w_out_attn.shape[1]
    heads = qw // HEAD_DIM
    kw = 2 * HEAD_DIM
    nw = qw + kw + 3 * cw
    chunk = rows // TP
    bf, f32 = jnp.bfloat16, jnp.float32
    dma = pltpu.SemaphoreType.DMA
    return pl.pallas_call(
        functools.partial(fused_kernel, Z, X),
        out_shape=(
            jax.ShapeDtypeStruct((chunk, S * cols), bf),
            jax.ShapeDtypeStruct((heads, rows), f32),
        ),
        in_specs=[pl.BlockSpec(memory_space=pltpu.VMEM)] * 11 + [pl.BlockSpec(memory_space=pltpu.SMEM)],
        out_specs=(pl.BlockSpec(memory_space=pltpu.VMEM),) * 2,
        scratch_shapes=[
            pltpu.VMEM((rows, kw), f32),
            pltpu.VMEM((rows, kw), f32),
            pltpu.VMEM((TP, rows, width), bf),
            pltpu.VMEM((rows, TP * width), bf),
            pltpu.VMEM((S, depth, nw), bf),
            pltpu.VMEM((S,) + w_out_attn.shape, bf),
            pltpu.VMEM((S,) + w_out_conv.shape, bf),
            pltpu.VMEM((rows, nw), f32),
            pltpu.VMEM((rows, qw), bf),
            pltpu.VMEM((rows + 2 * WINDOW, kw), bf),
            pltpu.VMEM((rows + 16, cw), f32),
            pltpu.VMEM((2, 16, cw), bf),
            pltpu.VMEM((2, 16, cw), bf),
            pltpu.VMEM((rows, qw), bf),
            pltpu.VMEM((rows, cw), bf),
            pltpu.VMEM((S, 2, chunk, cols), f32),
            pltpu.VMEM((S, 2, chunk, cols), bf),
            pltpu.VMEM((S, 2, chunk, cols), bf),
            pltpu.VMEM((S, chunk, cols), bf),
            pltpu.VMEM((S, chunk, cols), bf),
            dma((6,)),
            dma((3, 2, S)), dma((2, S)),
            dma((3, S)), dma((S,)),
            dma((3, S)), dma((S,)),
            dma((8,)),
            dma((4, S)),
            dma((4,)),
        ],
        compiler_params=pltpu.CompilerParams(
            collective_id=0, has_side_effects=True, vmem_limit_bytes=60 * 1024 * 1024
        ),
    )(
        tokens, norm_gain[None, :], w_query, w_key.T, w_value.T, w_post_gate, w_pre_gate, w_conv_in,
        w_out_attn, w_out_conv, conv_taps, sink_logit,
    )


def fits(
    tokens, norm_gain, w_query, w_key, w_value, w_post_gate, w_pre_gate, w_conv_in,
    conv_taps, sink_logit, w_out_attn, w_out_conv,
):
    S, TP = lax.axis_size("sp"), lax.axis_size("tp")
    return (
        TP == 4
        and S % 2 == 0
        and S >= 6
        and w_key.shape[1] == HEAD_DIM
        and w_query.shape[0] % 128 == 0
        and w_query.shape[1] % 128 == 0
        and w_post_gate.shape[1] % 128 == 0
        and w_out_attn.shape[1] % 128 == 0
        and tokens.shape[0] % (TP * WINDOW) == 0
        and tokens.shape[1] % 128 == 0
    )


def either(*args):
    return fused(*args) if fits(*args) else on_device(*args)


def solution(mesh):
    placed = (
        P("sp", "tp"),
        P(),
        P("sp", "tp"),
        P("sp", "tp"),
        P("sp", "tp"),
        P("sp", "tp"),
        P("sp", "tp"),
        P("sp", "tp"),
        P(None, "tp"),
        P("tp"),
        P("tp", "sp"),
        P("tp", "sp"),
    )
    return jax.shard_map(
        either,
        mesh=mesh,
        in_specs=placed,
        out_specs=(P(("sp", "tp"), None), P("tp", "sp")),
        check_vma=False,
    )
```
